32 devices in a mesh: sp: 8 (over z, x), tp: 4 (over y, core).
Axes of the slice: x: 2, y: 2, z: 4, core: 2. Of those that a mesh axis runs over, the one named last changes fastest.
Arguments:
- hidden_in: bfloat16 [3072, 2048], P('sp', 'tp'), may hold values from -6 to 6
- in_gain: float32 [2048], replicated, may hold values from 0.1 to 1.9
- receptance_weight: bfloat16 [2048, 1024], P(None, 'tp'), may hold values from -0.125 to 0.125
- key_weight: bfloat16 [2048, 1024], P(None, 'tp'), may hold values from -0.125 to 0.125
- value_weight: bfloat16 [2048, 1024], P(None, 'tp'), may hold values from -0.125 to 0.125
- decay_down: bfloat16 [2048, 128], replicated, may hold values from -0.125 to 0.125
- decay_up: bfloat16 [128, 1024], P(None, 'tp'), may hold values from -0.5 to 0.5
- decay_base: float32 [1024], P('tp'), may hold values from -14 to -2
- decay_shift: float32 [3072, 1024], P('sp', 'tp'), may hold values from -1 to 0
- learn_rate: float32 [1024], P('tp'), may hold values from 0 to 1
- query_pair: bfloat16 [2048, 8, 128], P(None, 'tp'), may hold values from -1 to 1
- key_pair: bfloat16 [2048, 8, 128], P(None, 'tp'), may hold values from -1 to 1
- value_pair: bfloat16 [2048, 8, 128], P(None, 'tp'), may hold values from -0.125 to 0.125
- mix_lambda: float32 [8], P('tp'), may hold values from 0.3 to 0.8
- out_recurrent: bfloat16 [1024, 2048], P('tp'), may hold values from -0.1875 to 0.1875
- out_attention: bfloat16 [1024, 2048], P('tp'), may hold values from -0.1875 to 0.1875
- out_gain: float32 [2048], replicated, may hold values from 0.1 to 1.9
Outputs:
- layer_out: bfloat16 [3072, 2048], P(('sp', 'tp'))
- log_sums: float32 [8, 2, 3072], P('tp', None, 'sp')
The draws below stay inside these ranges and needn't reach their ends.
All inputs are finite; a program needn't handle non-finite values.
Results may differ from the reference program's by a relative error of at most 0.018.
Values may be sent and summed in bfloat16 or wider, within the bound.
A program may use at most 128 MiB of HBM per device.

```python
import math
import jax
import jax.numpy as jnp
from jax import lax

D = 2048
RH = 16
DH = 8
HD = 64
LOW = 128
TOK_DEV = 384
TOKENS = 3072
RD = 1024
DW = 1024


def paired_maps(key):
    base = jax.random.fold_in(key, 101)
    leading = jax.random.normal(jax.random.fold_in(base, 1), (D, DH, 2 * HD), jnp.float32) * (3.0 / D) ** 0.5
    trailing = jax.random.normal(jax.random.fold_in(base, 2), (D, DH, 2 * HD), jnp.float32) * D ** (-0.5)
    return (jnp.clip(leading, -1.0, 1.0), jnp.clip(trailing, -1.0, 1.0))


def draw_query_pair(key, part):
    return paired_maps(key)[0].astype(jnp.bfloat16)


def draw_key_pair(key, part):
    return paired_maps(key)[1].astype(jnp.bfloat16)


def draw_hidden_in(key, part):
    rows = jax.random.normal(jax.random.fold_in(key, 7), (TOKENS, D), jnp.float32)
    return jnp.clip(rows, -6.0, 6.0).astype(jnp.bfloat16)


def draw_decay_base(key, part):
    base = jax.random.fold_in(key, 23)
    share = 0.5
    slow = jax.random.uniform(jax.random.fold_in(base, 1), (RH, 1), jnp.float32) < share
    slow_level = jnp.log(jax.random.uniform(jax.random.fold_in(base, 2), (RH, HD), jnp.float32, 0.05, 0.25) / TOKENS)
    fast_level = jax.random.uniform(jax.random.fold_in(base, 3), (RH, HD), jnp.float32, -3.5, -2.0)
    return jnp.where(slow, slow_level, fast_level).reshape(RH * HD)


def draw_decay_shift(key, part):
    base = jax.random.fold_in(key, 31)
    block_total = TOKENS // TOK_DEV
    rates = jnp.exp(jax.random.uniform(jax.random.fold_in(base, 1), (block_total, 1, 1), jnp.float32, math.log(0.1), math.log(0.4))) / TOKENS
    steady = jnp.broadcast_to(rates, (block_total, TOK_DEV, RH * HD)).reshape(TOKENS, RH * HD)
    places = jax.random.randint(jax.random.fold_in(base, 2), (3,), 0, TOKENS)
    sizes = jax.random.uniform(jax.random.fold_in(base, 3), (3, RH * HD), jnp.float32, 0.22, 0.3)
    hits = (jnp.arange(TOKENS)[:, None] == places[None, :]).astype(jnp.float32)
    return -(steady + jnp.dot(hits, sizes))


def draw_learn_rate(key, part):
    base = jax.random.fold_in(key, 41)
    weak_level = jax.random.uniform(jax.random.fold_in(base, 1), (RH * HD,), jnp.float32, math.log(4.0), math.log(40.0))
    weak = jnp.exp(weak_level) / TOKENS
    strong = jnp.exp(jax.random.uniform(jax.random.fold_in(base, 2), (RH * HD,), jnp.float32, math.log(0.05), math.log(0.8)))
    picked = jax.random.randint(jax.random.fold_in(base, 3), (RH * HD,), 0, 8) < 5
    return jnp.where(picked, strong, weak)


def block_levels(rng, dims, shards, smallest, top_value):
    def one(position, blocks):
        heights = jax.random.uniform(jax.random.fold_in(jax.random.fold_in(rng, 6), position), (blocks,), jnp.float32, smallest / len(shards), top_value / len(shards))
        return jnp.repeat(jnp.exp(heights), dims[position] // blocks).reshape((-1,) + (1,) * (len(dims) - position - 1))

    level = one(*shards[0])
    for cut in shards[1:]:
        level = level * one(*cut)
    return level


def bell_draw(key, dims, scale, reach, pieces=(), held_as=jnp.bfloat16):
    values = scale * jax.random.normal(key, dims, jnp.float32)
    if pieces:
        values = values * block_levels(key, dims, pieces, -0.22, 0.18)
    return jnp.clip(values, -reach, reach).astype(held_as)


def setup_inputs(seed: int = 0) -> dict:
    key_list = jax.random.split(jax.random.key(seed), 18)
    return {
        "hidden_in": draw_hidden_in(jax.random.fold_in(key_list[17], 71), 0),
        "in_gain": jnp.clip(1.0 + 0.18 * jax.random.normal(key_list[1], (D,), jnp.float32), 0.1, 1.9),
        "receptance_weight": bell_draw(key_list[2], (D, RD), D ** -0.5, 0.125, ((1, 4),)),
        "key_weight": bell_draw(key_list[3], (D, RD), D ** -0.5, 0.125, ((1, 4),)),
        "value_weight": bell_draw(key_list[4], (D, RD), D ** -0.5, 0.125, ((1, 4),)),
        "decay_down": bell_draw(key_list[5], (D, LOW), D ** -0.5, 0.125),
        "decay_up": bell_draw(key_list[6], (LOW, RD), LOW ** -0.5, 0.5, ((1, 4),)),
        "decay_base": draw_decay_base(jax.random.fold_in(key_list[17], 71), 0),
        "decay_shift": draw_decay_shift(jax.random.fold_in(key_list[17], 71), 0),
        "learn_rate": draw_learn_rate(jax.random.fold_in(key_list[17], 71), 0),
        "query_pair": draw_query_pair(jax.random.fold_in(key_list[17], 71), 0),
        "key_pair": draw_key_pair(jax.random.fold_in(key_list[17], 71), 0),
        "value_pair": bell_draw(key_list[12], (D, DH, 2 * HD), D ** -0.5, 0.125, ((1, 4),)),
        "mix_lambda": jnp.clip(0.3 + 0.5 * jax.random.uniform(key_list[13], (DH,), jnp.float32) ** block_levels(key_list[13], (DH,), ((0, 4),), -0.2, 0.2), 0.3, 0.8),
        "out_recurrent": bell_draw(key_list[14], (RD, D), RD ** -0.5, 0.1875, ((0, 4),)),
        "out_attention": bell_draw(key_list[15], (DW, D), DW ** -0.5, 0.1875, ((0, 4),)),
        "out_gain": jnp.clip(1.0 + 0.18 * jax.random.normal(key_list[16], (D,), jnp.float32), 0.1, 1.9),
    }


HIGHEST = lax.Precision.HIGHEST
DECAY_SCALE = math.exp(-0.5)
NORM_EPS = 1e-06
GROUP_EPS = 0.00064
HEAD_EPS = 1e-05
KEY_EPS = 1e-06

def rms_rows(values, gain):
    wide = values.astype(jnp.float32)
    return wide * lax.rsqrt(lax.optimization_barrier(jnp.mean(wide * wide, axis=-1, keepdims=True)) + NORM_EPS) * gain

def project(normed, weight):
    return jnp.dot(normed, weight.reshape(D, -1), preferred_element_type=jnp.float32).astype(jnp.bfloat16)

def recurrence(receptance, key_rows, value_rows, log_decay, learn_rate):
    shape = (TOKENS, RH, HD)
    receptance = receptance.astype(jnp.float32).reshape(shape)
    key_rows = key_rows.astype(jnp.float32).reshape(shape)
    value_rows = value_rows.astype(jnp.float32).reshape(shape)
    decay = jnp.exp(log_decay).reshape(shape)
    unit_keys = key_rows * lax.rsqrt(lax.optimization_barrier(jnp.sum(key_rows * key_rows, axis=-1, keepdims=True)) + KEY_EPS)
    erasing = unit_keys * learn_rate.reshape(RH, HD)

    def advance(carried, inputs):
        read_now, decay_now, key_now, value_now, unit_now, erase_now = inputs
        removed = jnp.einsum('hvk,hk->hv', carried, unit_now, precision=HIGHEST)
        carried = carried * decay_now[:, None, :] - removed[:, :, None] * erase_now[:, None, :] + value_now[:, :, None] * key_now[:, None, :]
        return (carried, jnp.einsum('hvk,hk->hv', carried, read_now, precision=HIGHEST))
    initial = jnp.zeros((RH, HD, HD), jnp.float32)
    outputs = lax.scan(advance, initial, (receptance, decay, key_rows, value_rows, unit_keys, erasing))[1]
    centered = outputs - lax.optimization_barrier(jnp.mean(outputs, axis=-1, keepdims=True))
    normal = centered * lax.rsqrt(lax.optimization_barrier(jnp.mean(centered * centered, axis=-1, keepdims=True)) + GROUP_EPS)
    return normal.reshape(TOKENS, RH * HD).astype(jnp.bfloat16)

def differential(queries, pair_keys, pair_values, mix_lambda):
    places = jnp.arange(TOKENS)
    score_scale = HD ** (-0.5)
    block_count = TOKENS // TOK_DEV

    def one_head(inputs):
        head_queries, head_keys, head_values, head_lambda = inputs
        keys_wide = head_keys.astype(jnp.float32).reshape(TOKENS, 2, HD)
        values_wide = head_values.astype(jnp.float32)
        query_blocks = head_queries.reshape(block_count, TOK_DEV, 2, HD)

        def one_block(block_inputs):
            block_queries, block_number = block_inputs
            rows_at = block_number * TOK_DEV + jnp.arange(TOK_DEV)
            scores = jnp.einsum('qmd,kmd->mqk', block_queries.astype(jnp.float32), keys_wide) * score_scale
            allowed = rows_at[:, None] >= places[None, :]
            scores = jnp.where(allowed[None], scores, -jnp.inf)
            row_max = lax.optimization_barrier(jnp.max(scores, axis=-1, keepdims=True))
            weights = jnp.exp(scores - row_max)
            row_sum = lax.optimization_barrier(jnp.sum(weights, axis=-1, keepdims=True))
            rounded = lax.optimization_barrier(weights.astype(jnp.bfloat16)).astype(jnp.float32)
            map_out = jnp.einsum('mqk,kv->mqv', rounded, values_wide) / row_sum
            head_out = map_out[0] - head_lambda * map_out[1]
            head_out = head_out * lax.rsqrt(lax.optimization_barrier(jnp.mean(head_out * head_out, axis=-1, keepdims=True)) + HEAD_EPS)
            return (head_out, (row_max + jnp.log(row_sum))[..., 0])
        outs, sums = lax.map(one_block, (query_blocks, jnp.arange(block_count)))
        return (outs.reshape(TOKENS, 2 * HD), sums.transpose(1, 0, 2).reshape(2, TOKENS))
    head_outs, log_sums = lax.map(one_head, (queries.transpose(1, 0, 2), pair_keys.transpose(1, 0, 2), pair_values.transpose(1, 0, 2), mix_lambda))
    att_mix = head_outs.transpose(1, 0, 2).reshape(TOKENS, DH * 2 * HD).astype(jnp.bfloat16)
    return (att_mix, log_sums)

def reference(hidden_in, in_gain, receptance_weight, key_weight, value_weight, decay_down, decay_up, decay_base, decay_shift, learn_rate, query_pair, key_pair, value_pair, mix_lambda, out_recurrent, out_attention, out_gain):
    normed = rms_rows(hidden_in, in_gain).astype(jnp.bfloat16)
    receptance = project(normed, receptance_weight)
    rec_keys = project(normed, key_weight)
    rec_values = project(normed, value_weight)
    low_rank = jnp.tanh(jnp.dot(normed, decay_down, preferred_element_type=jnp.float32)).astype(jnp.bfloat16)
    log_decay = -DECAY_SCALE * jax.nn.sigmoid(jnp.dot(low_rank, decay_up, preferred_element_type=jnp.float32) + decay_base) + decay_shift
    rec_mix = recurrence(receptance, rec_keys, rec_values, log_decay, learn_rate)
    queries = project(normed, query_pair).reshape(TOKENS, DH, 2 * HD)
    pair_keys = project(normed, key_pair).reshape(TOKENS, DH, 2 * HD)
    pair_values = project(normed, value_pair).reshape(TOKENS, DH, 2 * HD)
    att_mix, log_sums = differential(queries, pair_keys, pair_values, mix_lambda)
    projected = jnp.dot(rec_mix, out_recurrent, preferred_element_type=jnp.float32) + jnp.dot(att_mix, out_attention, preferred_element_type=jnp.float32)
    return (rms_rows(projected, out_gain).astype(jnp.bfloat16), log_sums)
```

```python
import functools
import math

import jax
import jax.numpy as jnp
from jax import lax
from jax.experimental import pallas as pl
from jax.experimental.pallas import tpu as pltpu
from jax.sharding import PartitionSpec as P

HD = 64
LANES = 128
CHUNK = 64
DECAY_SCALE = math.exp(-0.5)
NORM_EPS = 1e-06
GROUP_EPS = 0.00064
HEAD_EPS = 1e-05
KEY_EPS = 1e-06
NEGATIVE = -1e30
F32 = jnp.float32
BF16 = jnp.bfloat16

NN = (((1,), (0,)), ((), ()))
NT = (((1,), (1,)), ((), ()))
TN = (((0,), (0,)), ((), ()))


def dot1(a, b, dims=NN):
    return lax.dot_general(a.astype(BF16), b.astype(BF16), dims, preferred_element_type=F32)


def halves(a):
    high = a.astype(BF16)
    return high, (a - high.astype(F32)).astype(BF16)


def dot3(a, b, dims=NN):
    ah, al = halves(a)
    bh, bl = halves(b)
    one = functools.partial(lax.dot_general, dimension_numbers=dims, preferred_element_type=F32)
    return one(ah, bh) + (one(al, bh) + one(ah, bl))


def swapped(place, turn):
    bit = 1
    while bit <= turn:
        if turn & bit:
            place = place + bit - 2 * bit * lax.rem(lax.div(place, bit), 2)
        bit *= 2
    return place


def normalize(pieces, gain, normed, me, here):
    count = len(pieces)
    width = pieces[0].shape[1]
    wides = [piece[here, :].astype(F32) for piece in pieces]
    total = sum(jnp.sum(wide * wide, axis=-1, keepdims=True) for wide in wides)
    scale = lax.rsqrt(total / (width * count) + NORM_EPS)
    for turn, wide in enumerate(wides):
        columns = pl.ds(pl.multiple_of(swapped(me, turn) * width, LANES), width)
        normed[here, columns] = (wide * scale * gain[:, columns]).astype(BF16)


def recurrent_body(group, between, r_ref, k_ref, v_ref, d_ref, learn_ref, out_ref, turn_ref, end_ref, state):
    rows, features = r_ref.shape
    pairs = features // LANES
    lane = lax.broadcasted_iota(jnp.int32, (1, LANES), 1)
    first = (lane < HD).astype(F32)
    second = 1.0 - first
    line = lax.broadcasted_iota(jnp.int32, (LANES, LANES), 0)
    column = lax.broadcasted_iota(jnp.int32, (LANES, LANES), 1)
    strict = line > column
    causal = line >= column
    eye = (line == column).astype(F32)
    same_head = ((line // HD) == (column // HD)).astype(BF16)
    small_line = lax.broadcasted_iota(jnp.int32, (CHUNK, CHUNK), 0)
    small_column = lax.broadcasted_iota(jnp.int32, (CHUNK, CHUNK), 1)
    lower = (small_line >= small_column).astype(BF16)

    def below(size):
        return ((line // size) == (column // size) + 1) & ((line // size) % 2 == 1)

    def spread(x):
        return jnp.concatenate([x * first, x * second], axis=0)

    for pair in range(pairs):
        state[pair, :LANES, :] = jnp.zeros((LANES, LANES), F32)
        state[pair, LANES:, :] = eye

    def local(pair, at):
        here = (pl.ds(at, CHUNK), pl.ds(pair * LANES, LANES))
        r = r_ref[here].astype(F32)
        k = k_ref[here].astype(F32)
        v = v_ref[here].astype(F32)
        decay = d_ref[here]
        learn = learn_ref[:, pl.ds(pair * LANES, LANES)]
        dh = decay.astype(BF16)
        rest = decay - dh.astype(F32)
        dm = rest.astype(BF16)
        dl = (rest - dm.astype(F32)).astype(BF16)
        running = dot1(lower, dh) + (dot1(lower, dm) + dot1(lower, dl))
        before = running - decay
        middle = running[CHUNK // 2 - 1 : CHUNK // 2, :]
        ending = running[CHUNK - 1 :, :]
        sh, sl = halves(k * k)
        squares = dot1(sh, same_head) + dot1(sl, same_head)
        unit = k * lax.rsqrt(squares + KEY_EPS)
        erase = unit * learn
        rise = jnp.exp(middle - running)
        left = jnp.concatenate(
            [spread(-unit * jnp.exp(before - middle)), spread(r * jnp.exp(running - middle))], axis=0
        )
        right = jnp.concatenate([spread(erase * rise), spread(k * rise)], axis=0)
        to_end = jnp.exp(ending - running)
        return dict(
            left=left,
            right=right,
            against=spread(-unit * jnp.exp(before)),
            read=spread(r * jnp.exp(running)),
            erase_end=spread(erase * to_end),
            keys_end=spread(k * to_end),
            values=spread(v),
            whole=jnp.exp(ending),
        )

    def step(turn, carry):
        between(turn)
        spots = [(turn * group + g, pair) for g in range(group) for pair in range(pairs)]
        items = [local(pair, pl.multiple_of(c * CHUNK, CHUNK)) for c, pair in spots]
        for it in items:
            scores = dot3(it["left"], it["right"], NT)
            it["low"] = jnp.where(strict, scores[:LANES, :LANES], 0.0)
            it["carry"] = jnp.where(strict, scores[:LANES, LANES:], 0.0)
            it["read_erase"] = jnp.where(causal, scores[LANES:, :LANES], 0.0)
            it["read_keys"] = jnp.where(causal, scores[LANES:, LANES:], 0.0)
            it["inv"] = eye + jnp.where(below(1), it["low"], 0.0)
        size = 2
        while size < CHUNK:
            keep = below(size)
            for it in items:
                it["mid"] = dot3(jnp.where(keep, it["low"], 0.0), it["inv"])
            for it in items:
                it["inv"] = it["inv"] + dot3(it["inv"], it["mid"])
            size *= 2
        for it in items:
            it["fed"] = dot3(it["carry"], it["values"])
        for it in items:
            side = jnp.concatenate([it["against"], it["fed"]], axis=1)
            it["solved"] = dot3(it["inv"], side)
        for it in items:
            seen = dot1(it["read_erase"], it["solved"])
            it["heard"] = seen[:, LANES:] + dot1(it["read_keys"], it["values"])
            it["read"] = it["read"] + seen[:, :LANES]
            it["added"] = dot3(it["values"], it["keys_end"], TN)
        for (c, pair), it in zip(spots, items):
            now = state[pair]
            both = jnp.concatenate([it["solved"][:, :LANES], it["read"]], axis=0)
            met = dot3(both, now, NT)
            gone = jnp.concatenate(
                [met[:LANES, :LANES] + it["solved"][:, LANES:], met[:LANES, LANES:]], axis=1
            )
            later = now * it["whole"] + dot3(gone, it["erase_end"], TN)
            state[pair, :LANES, :] = later[:LANES] + it["added"]
            state[pair, LANES:, :] = later[LANES:]
            heard = met[LANES:, :LANES] + it["heard"]
            turned = met[LANES:, LANES:]
            here = (pl.ds(pl.multiple_of(c * CHUNK, CHUNK), CHUNK), pl.ds(pair * LANES, LANES))
            out_ref[here] = heard[:CHUNK] + heard[CHUNK:]
            turn_ref[here] = turned[:CHUNK] + turned[CHUNK:]
        return carry

    lax.fori_loop(0, rows // CHUNK // group, step, 0)
    for pair in range(pairs):
        now = state[pair]
        end_ref[pair, :HD, :] = (now[:HD] + now[HD:LANES]).astype(BF16)
        end_ref[pair, HD:, :] = (now[LANES : LANES + HD] + now[LANES + HD :]).astype(BF16)


def finish_body(out_ref, turn_ref, ends, place, mix_ref):
    pairs = out_ref.shape[1] // LANES
    lane = lax.broadcasted_iota(jnp.int32, (1, LANES), 1)
    first = (lane < HD).astype(F32)
    second = 1.0 - first
    line = lax.broadcasted_iota(jnp.int32, (LANES, LANES), 0)
    column = lax.broadcasted_iota(jnp.int32, (LANES, LANES), 1)
    same_head = ((line // HD) == (column // HD)).astype(BF16)

    def spread(x):
        return jnp.concatenate([x * first, x * second], axis=0)

    for pair in range(pairs):
        entering = jnp.zeros((LANES, LANES), F32)
        for far, end in ends:
            block = jnp.where(place >= far, end[pair].astype(F32), 0.0)
            high, low = halves(entering)
            move = spread(block[HD:])
            entering = dot1(high, move) + dot1(low, move) + spread(block[:HD])
        columns = pl.ds(pair * LANES, LANES)
        full = out_ref[:, columns] + dot3(turn_ref[:, columns], entering, NT)

        def mean(x):
            high, low = halves(x)
            return (dot1(high, same_head) + dot1(low, same_head)) * (1.0 / HD)

        centered = full - mean(full)
        mix_ref[pair] = (centered * lax.rsqrt(mean(centered * centered) + GROUP_EPS)).astype(
            BF16
        )


def update(queries, at, tile, blocks, mask, tops, sums, accs):
    here = pl.ds(2 * at, 2 * tile)
    lhs = queries[here, :]
    scores = [
        lax.dot_general(lhs, keys, NT, preferred_element_type=F32) for keys, _ in blocks
    ]
    if mask is not None:
        scores = [jnp.where(mask, s, NEGATIVE) for s in scores]
    old = tops[here, :]
    top = functools.reduce(jnp.maximum, [jnp.max(s, axis=-1, keepdims=True) for s in scores])
    top = jnp.maximum(top, old)
    fade = jnp.exp(old - top)
    row_sum = sums[here, :] * fade
    acc = accs[here, :] * fade
    for s, (_, values) in zip(scores, blocks):
        weights = jnp.exp(s - top)
        row_sum = row_sum + jnp.sum(weights, axis=-1, keepdims=True)
        acc = acc + jnp.dot(weights.astype(BF16), values, preferred_element_type=F32)
    return here, top, row_sum, acc


def attend(q, kv, head, index, lam, queries, tops, sums, accs, mix_ref, log_ref):
    rows = q.shape[0]
    tile = LANES if rows % LANES == 0 else rows
    starts = range(0, rows, tile)
    lane = lax.broadcasted_iota(jnp.int32, (1, LANES), 1)
    for at in starts:
        part = q[pl.ds(at, tile), :].astype(F32) * HD ** (-0.5)
        queries[pl.ds(2 * at, 2 * tile), :] = jnp.concatenate(
            [jnp.where(lane < HD, part, 0.0), jnp.where(lane < HD, 0.0, part)], axis=0
        ).astype(BF16)
    tops[...] = jnp.full(tops.shape, NEGATIVE, F32)
    sums[...] = jnp.zeros(sums.shape, F32)
    accs[...] = jnp.zeros(accs.shape, F32)

    def fold(numbers):
        blocks = [(kv[n, head, :, :LANES], kv[n, head, :, LANES:]) for n in numbers]
        for at in starts:
            here, top, row_sum, acc = update(
                queries, at, tile, blocks, None, tops, sums, accs
            )
            tops[here, :] = top
            sums[here, :] = row_sum
            accs[here, :] = acc

    def both(turn, carry):
        fold([2 * turn, 2 * turn + 1])
        return carry

    lax.fori_loop(0, lax.div(index, 2), both, 0)
    pl.when(lax.rem(index, 2) == 1)(lambda: fold([index - 1]))
    for at in starts:
        size = at + tile
        line = lax.broadcasted_iota(jnp.int32, (tile, size), 0) + at
        seen = line >= lax.broadcasted_iota(jnp.int32, (tile, size), 1)
        block = (kv[index, head, :size, :LANES], kv[index, head, :size, LANES:])
        mask = jnp.concatenate([seen, seen], axis=0)
        _, top, row_sum, acc = update(queries, at, tile, [block], mask, tops, sums, accs)
        maps = acc / row_sum
        logs = top + jnp.log(row_sum)
        flat = jnp.transpose(jnp.broadcast_to(logs, (2 * tile, LANES)))
        log_ref[0:1, pl.ds(at, tile)] = flat[:1, :tile]
        log_ref[1:2, pl.ds(at, tile)] = flat[:1, tile:]
        out = maps[:tile] - lam * maps[tile:]
        out = out * lax.rsqrt(jnp.mean(out * out, axis=-1, keepdims=True) + HEAD_EPS)
        mix_ref[pl.ds(at, tile), :] = out.astype(BF16)


def layer_body(sp, tp, *refs):
    (hidden, gain, wr_h, wk_h, wv_h, down_h, up_h, base, shift, learn) = refs[:10]
    (wq_h, wkp_h, wvp_h, lam, rec_h, att_h, out_gain, out, logs) = refs[10:19]
    (xs, normed, wr, wk, wv, down, up, wq, wkp, wvp, hw) = refs[19:30]
    (wq_p, wkp_p, wvp_p, kv, r, k, v, d, q, heard, turned, ends, state) = refs[30:43]
    (queries, top, row_sum, acc, mix, moved, q_far, mix_far, log_far) = refs[43:52]
    (log_got, total, parts, got) = refs[52:56]
    (load, x_send, x_recv, w_send, w_recv, z_send, z_recv, c_send, c_recv) = refs[56:65]
    (e_send, e_recv, q_send, q_recv, b_send, b_recv, m_send, m_recv) = refs[65:73]
    (p_send, p_recv) = refs[73:]
    rows, features = r.shape
    heads = q.shape[0]
    wide = heads * LANES
    pairs = features // LANES
    me = lax.axis_index("tp")
    place = lax.axis_index("sp")
    count = sp // 2
    level = lax.div(place, 2)
    across = swapped(place, 1)
    mirror = sp - 1 - place
    early = place < count
    late = place >= count
    moving = list(range(heads - heads // 2, heads))
    staying = list(range(heads - heads // 2))
    parts_of = z_recv.shape[2]
    piece = rows // parts_of

    barrier = pltpu.get_barrier_semaphore()
    for turn in range(1, tp):
        pl.semaphore_signal(barrier, inc=1, device_id={"tp": swapped(me, turn)})
    for hop in range(1, sp):
        pl.semaphore_signal(barrier, inc=1, device_id={"sp": lax.rem(place + hop, sp)})
    pair_loads = heads > 1
    loads = []
    for number, (source, target) in enumerate(
        (
            (wkp_h, wkp_p if pair_loads else wkp),
            (wvp_h, wvp_p if pair_loads else wvp),
            (wq_h, wq_p if pair_loads else wq),
            (wr_h, wr),
            (wk_h, wk),
            (wv_h, wv),
            (down_h, down),
            (up_h, up),
            (rec_h, hw.at[0, pl.ds(0, features)]),
            (att_h, hw.at[0, pl.ds(features, wide)]),
        )
    ):
        loads.append(pltpu.make_async_copy(source, target, load.at[number]))
        loads[-1].start()
    pl.semaphore_wait(barrier, tp - 1 + sp - 1)

    def remote(source, target, send, recv, device):
        return pltpu.make_async_remote_copy(
            src_ref=source, dst_ref=target, send_sem=send, recv_sem=recv, device_id=device
        )

    chunks = [pl.ds(number * piece, piece) for number in range(parts_of)]
    hops = {}
    for turn in range(1, tp):
        for number, here in enumerate(chunks):
            source = hidden if turn < 2 or turn % 2 == 0 else xs.at[turn - 1]
            hops[turn, number] = remote(
                source.at[here],
                xs.at[turn, here],
                x_send.at[turn, number],
                x_recv.at[turn, number],
                {"tp": swapped(me, turn if turn % 2 == 0 else 1)},
            )
    for number in range(parts_of):
        for turn in range(2, tp, 2):
            hops[turn, number].start()
        hops[1, number].start()

    def unpack(packed, target):
        def one(turn, carry):
            lines = pl.ds(pl.multiple_of(turn * 256, 256), 256)
            for head in range(heads):
                target[lines, pl.ds(head * LANES, LANES)] = packed[lines, head, :]
            return carry

        lax.fori_loop(0, target.shape[0] // 256, one, 0)

    for one in loads[:3]:
        one.wait()
    if pair_loads:
        unpack(wkp_p, wkp)
        unpack(wvp_p, wvp)
        unpack(wq_p, wq)

    def column(head, source, target, number):
        here = kv.at[source, head, chunks[number]]
        return remote(
            here,
            here,
            z_send.at[head, target, number],
            z_recv.at[head, source_level(source), number],
            {"sp": 2 * target + lax.rem(place, 2)},
        )

    def source_level(source):
        return lax.div(source, 2)

    def crossing(head, source, number):
        here = kv.at[source, head, chunks[number]]
        return remote(
            here,
            here,
            c_send.at[head, source_level(source), number],
            c_recv.at[head, source_level(source), number],
            {"sp": across},
        )

    def column_goes():
        plan = []
        for target in range(count - 1, -1, -1):
            for head in staying:
                plan.append((head, target, target > level))
            if target < count // 2:
                for head in moving:
                    plan.append((head, target, (target != level) & (level <= count - 1 - target)))
        return plan

    own_crosses = [(head, lax.rem(place, 2) == 0) for head in staying] + [
        (head, level < count // 2) for head in moving
    ]
    relayed = []
    for far in range(1, count):
        stage = []
        for head in staying:
            stage.append((head, level - far, level >= far))
        for head in moving:
            stage.append(
                (head, level + far, (level < count // 2) & (level + far <= count - 1 - level))
            )
            stage.append((head, level - far, (level < count // 2) & (level >= far)))
        relayed.append(stage)

    def guarded(condition, work):
        pl.when(condition)(work)

    def send_piece(number):
        for head, condition in own_crosses:
            guarded(condition, lambda head=head: crossing(head, place, number).start())
        for head, target, condition in column_goes():
            guarded(
                condition,
                lambda head=head, target=target: column(head, place, target, number).start(),
            )

    def relay(stage):
        for head, source, condition in relayed[stage]:

            def one(head=head, source=source):
                slot = 2 * source + lax.rem(place, 2)
                for number in range(parts_of):
                    column(head, slot, level, number).wait_recv()
                    crossing(head, slot, number).start()

            guarded(condition, one)

    def product(here, weight):
        return jnp.dot(normed[here, :], weight[...], preferred_element_type=F32)

    for number, here in enumerate(chunks):
        for turn in range(2, tp, 2):
            hops[turn, number].wait_recv()
            hops[turn + 1, number].start()
        for turn in range(1, tp, 2):
            hops[turn, number].wait_recv()
        normalize([hidden] + [xs.at[turn] for turn in range(1, tp)], gain, normed, me, here)
        keys = product(here, wkp).astype(BF16)
        values = product(here, wvp).astype(BF16)
        for head in range(heads):
            columns = slice(head * LANES, (head + 1) * LANES)
            kv[place, head, here, :LANES] = keys[:, columns]
            kv[place, head, here, LANES:] = values[:, columns]
        send_piece(number)
        if number == 0:
            for one in loads[3:]:
                one.wait()
            outs = remote(
                hw.at[0], hw.at[1], w_send.at[0], w_recv.at[0], {"tp": swapped(me, 1)}
            )
            outs.start()
        mine = product(here, wq).astype(BF16)
        for head in range(heads):
            q[head, here, :] = mine[:, head * LANES : (head + 1) * LANES]
        r[here, :] = product(here, wr).astype(BF16)
        k[here, :] = product(here, wk).astype(BF16)
        v[here, :] = product(here, wv).astype(BF16)
        low_rank = jnp.tanh(product(here, down)).astype(BF16)
        pre = jnp.dot(low_rank, up[...], preferred_element_type=F32) + base[...]
        d[here, :] = -DECAY_SCALE * jax.nn.sigmoid(pre) + shift[here, :]

    asks = [
        remote(q.at[head], q_far.at[n], q_send.at[n], q_recv.at[n], {"sp": mirror})
        for n, head in enumerate(moving)
    ]
    if moving:
        guarded(late, lambda: [one.start() for one in asks] and None)

    group = 2 if (rows // CHUNK) % 2 == 0 else 1
    turns = rows // CHUNK // group
    placed = {}
    for stage in range(count - 1):
        placed.setdefault(min(stage + 1, turns), []).append(stage)

    def between(turn):
        for when, stages in placed.items():
            if when < turns:

                def work(stages=stages):
                    for stage in stages:
                        relay(stage)

                pl.when(turn == when)(work)

    recurrent_body(group, between, r, k, v, d, learn, heard, turned, ends.at[0], state)
    states = {
        hop: remote(
            ends.at[0], ends.at[hop], e_send.at[hop], e_recv.at[hop], {"sp": place + hop}
        )
        for hop in range(1, sp)
    }
    for hop in range(1, sp):
        guarded(place + hop < sp, states[hop].start)
    for stage in placed.get(turns, []):
        relay(stage)

    def arrive(names, last):
        for source in range(count):
            for side in range(2):
                slot = 2 * source + side

                def one(slot=slot):
                    for head in names:
                        for number in range(parts_of):
                            crossing(head, slot, number).wait_recv()

                guarded((lax.rem(place, 2) != side) & (slot <= last), one)

    answers = []
    for n, head in enumerate(moving):
        answers.append(
            remote(
                mix_far.at[n],
                mix.at[pairs + head],
                b_send.at[n, 0],
                b_recv.at[n, 0],
                {"sp": mirror},
            )
        )
        answers.append(
            remote(
                log_far.at[n], log_got.at[n], b_send.at[n, 1], b_recv.at[n, 1], {"sp": mirror}
            )
        )
    work = (queries, top, row_sum, acc)

    if moving:

        def foreign():
            arrive(moving, mirror)
            for n, head in enumerate(moving):
                asks[n].wait_recv()
                attend(
                    q_far.at[n], kv, head, mirror, lam[head], *work, mix_far.at[n], log_far.at[n]
                )
                answers[2 * n].start()
                answers[2 * n + 1].start()

        guarded(early, foreign)
    arrive(staying, place)
    for head in staying:
        attend(
            q.at[head], kv, head, place, lam[head], *work, mix.at[pairs + head], logs.at[head]
        )
    if moving:

        def local():
            for head in moving:
                attend(
                    q.at[head],
                    kv,
                    head,
                    place,
                    lam[head],
                    *work,
                    mix.at[pairs + head],
                    logs.at[head],
                )

        guarded(early, local)
    for hop in range(1, sp):
        guarded(place >= hop, states[hop].wait_recv)
    finish_body(
        heard, turned, [(hop, ends.at[hop]) for hop in range(sp - 1, 0, -1)], place, mix
    )
    if moving:

        def collect():
            for one in answers:
                one.wait_recv()
            for n, head in enumerate(moving):
                logs[head] = log_got[n]

        guarded(late, collect)

    part = rows // tp
    mate = swapped(me, 1)

    def lines(owner):
        return pl.ds(pl.multiple_of(owner * part, part), part)

    swaps = []
    for turn in range(tp // 2):
        theirs = lines(lax.rem(mate + 2 * turn, tp))
        swaps.append(
            remote(
                mix.at[:, theirs],
                moved.at[:, theirs],
                m_send.at[turn],
                m_recv.at[turn],
                {"tp": mate},
            )
        )
    for one in swaps:
        one.start()
    owners = [lax.rem(me + 2 * turn, tp) for turn in range(1, tp // 2)] + [me]
    outs.wait_recv()
    blocks = pairs + heads
    for one in swaps:
        one.wait_recv()
    near = jnp.concatenate(
        [
            jnp.concatenate([mix[b, lines(owner), :] for b in range(blocks)], axis=1)
            for owner in owners
        ],
        axis=0,
    )
    far = jnp.concatenate(
        [
            jnp.concatenate([moved[b, lines(owner), :] for b in range(blocks)], axis=1)
            for owner in owners
        ],
        axis=0,
    )
    slabs, slab = parts.shape[1], parts.shape[3]
    trades = {}
    for number in range(slabs):
        columns = pl.ds(number * slab, slab)
        result = jnp.dot(near, hw[0, :, columns], preferred_element_type=F32)
        result = result + jnp.dot(far, hw[1, :, columns], preferred_element_type=F32)
        for turn in range(1, tp // 2):
            parts[turn, number] = result[(turn - 1) * part : turn * part].astype(BF16)
            trades[turn, number] = remote(
                parts.at[turn, number],
                got.at[turn, number],
                p_send.at[turn, number],
                p_recv.at[turn, number],
                {"tp": lax.rem(me + 2 * turn, tp)},
            )
            trades[turn, number].start()
        total[:, columns] = result[(tp // 2 - 1) * part :]
    for number in range(slabs):
        columns = pl.ds(number * slab, slab)
        full = total[:, columns]
        for turn in range(1, tp // 2):
            trades[turn, number].wait_recv()
            full = full + got[turn, number].astype(F32)
        total[:, columns] = full
    full = total[...]
    mean = jnp.mean(full * full, axis=-1, keepdims=True)
    out[...] = (full * lax.rsqrt(mean + NORM_EPS) * out_gain[...]).astype(BF16)

    for group_of in (hops, trades):
        for one in group_of.values():
            one.wait_send()
    for one in swaps:
        one.wait_send()
    outs.wait_send()
    for number in range(parts_of):
        for head, condition in own_crosses:
            guarded(condition, crossing(head, place, number).wait_send)
        for head, target, condition in column_goes():
            guarded(condition, column(head, place, target, number).wait_send)
    for stage in relayed:
        for head, source, condition in stage:

            def one(head=head, source=source):
                for number in range(parts_of):
                    crossing(head, 2 * source + lax.rem(place, 2), number).wait_send()

            guarded(condition, one)
    for hop in range(1, sp):
        guarded(place + hop < sp, states[hop].wait_send)
    if moving:
        guarded(late, lambda: [one.wait_send() for one in asks] and None)
        guarded(early, lambda: [one.wait_send() for one in answers] and None)


def per_device(
    sp,
    tp,
    hidden_in,
    in_gain,
    receptance_weight,
    key_weight,
    value_weight,
    decay_down,
    decay_up,
    decay_base,
    decay_shift,
    learn_rate,
    query_pair,
    key_pair,
    value_pair,
    mix_lambda,
    out_recurrent,
    out_attention,
    out_gain,
):
    rows, width = hidden_in.shape
    depth = width * tp
    features = receptance_weight.shape[1]
    heads = mix_lambda.shape[0]
    wide = heads * LANES
    pairs = features // LANES
    low = decay_down.shape[1]
    across = out_recurrent.shape[1]
    part = rows // tp
    count = sp // 2
    movers = max(heads // 2, 1)
    pieces = rows // LANES if rows % LANES == 0 else 1
    slabs = 4 if across % (4 * LANES) == 0 else 1
    shape = jax.ShapeDtypeStruct
    held = pltpu.VMEM

    def paired(weight):
        return weight if heads > 1 else weight.reshape(depth, wide)

    args = (
        hidden_in,
        in_gain.reshape(1, -1),
        receptance_weight,
        key_weight,
        value_weight,
        decay_down,
        decay_up,
        decay_base.reshape(1, -1),
        decay_shift,
        learn_rate.reshape(1, -1),
        paired(query_pair),
        paired(key_pair),
        paired(value_pair),
        mix_lambda,
        out_recurrent,
        out_attention,
        out_gain.reshape(1, -1),
    )
    inside = pl.BlockSpec(memory_space=pltpu.VMEM)
    outside = pl.BlockSpec(memory_space=pl.ANY)
    specs = [inside] * 2 + [outside] * 5 + [inside] * 3 + [outside] * 3
    specs += [pl.BlockSpec(memory_space=pltpu.SMEM)] + [outside] * 2 + [inside]
    raw = (depth, heads, LANES) if heads > 1 else (8, LANES)
    sizes = ((10,), (tp, pieces), (tp, pieces), (1,), (1,))
    sizes += ((heads, count, pieces),) * 4
    sizes += ((sp,), (sp,), (movers,), (movers,), (movers, 2), (movers, 2))
    sizes += ((tp // 2,), (tp // 2,), (tp // 2, slabs), (tp // 2, slabs))
    return tuple(
        pl.pallas_call(
            functools.partial(layer_body, sp, tp),
            out_shape=[shape((part, across), BF16), shape((heads, 2, rows), F32)],
            in_specs=specs,
            out_specs=[inside] * 2,
            scratch_shapes=[
                held((tp, rows, width), BF16),
                held((rows, depth), BF16),
                held((depth, features), BF16),
                held((depth, features), BF16),
                held((depth, features), BF16),
                held((depth, low), BF16),
                held((low, features), BF16),
                held((depth, wide), BF16),
                held((depth, wide), BF16),
                held((depth, wide), BF16),
                held((2, features + wide, across), BF16),
                held(raw, BF16),
                held(raw, BF16),
                held(raw, BF16),
                held((sp, heads, rows, 2 * LANES), BF16),
                held((rows, features), BF16),
                held((rows, features), BF16),
                held((rows, features), BF16),
                held((rows, features), F32),
                held((heads, rows, LANES), BF16),
                held((rows, features), F32),
                held((rows, features), F32),
                held((sp, pairs, 2 * HD, LANES), BF16),
                held((pairs, 2 * LANES, LANES), F32),
                held((2 * rows, LANES), BF16),
                held((2 * rows, 1), F32),
                held((2 * rows, 1), F32),
                held((2 * rows, LANES), F32),
                held((pairs + heads, rows, LANES), BF16),
                held((pairs + heads, rows, LANES), BF16),
                held((movers, rows, LANES), BF16),
                held((movers, rows, LANES), BF16),
                held((movers, 2, rows), F32),
                held((movers, 2, rows), F32),
                held((part, across), F32),
                held((tp // 2, slabs, part, across // slabs), BF16),
                held((tp // 2, slabs, part, across // slabs), BF16),
            ]
            + [pltpu.SemaphoreType.DMA(size) for size in sizes],
            compiler_params=pltpu.CompilerParams(
                collective_id=0, has_side_effects=True, vmem_limit_bytes=62 * 1024 * 1024
            ),
        )(*args)
    )


def solution(mesh):
    in_specs = (
        P("sp", "tp"),
        P(),
        P(None, "tp"),
        P(None, "tp"),
        P(None, "tp"),
        P(),
        P(None, "tp"),
        P("tp"),
        P("sp", "tp"),
        P("tp"),
        P(None, "tp", None),
        P(None, "tp", None),
        P(None, "tp", None),
        P("tp"),
        P("tp", None),
        P("tp", None),
        P(),
    )
    out_specs = (P(("sp", "tp"), None), P("tp", None, "sp"))
    body = functools.partial(per_device, mesh.shape["sp"], mesh.shape["tp"])
    return jax.shard_map(
        body, mesh=mesh, in_specs=in_specs, out_specs=out_specs, check_vma=False
    )
```

```python
import functools
import math

import jax
import jax.numpy as jnp
from jax import lax
from jax.experimental import pallas as pl
from jax.experimental.pallas import tpu as pltpu
from jax.sharding import PartitionSpec as P

HD = 64
LANES = 128
CHUNK = 64
DECAY_SCALE = math.exp(-0.5)
NORM_EPS = 1e-06
GROUP_EPS = 0.00064
HEAD_EPS = 1e-05
KEY_EPS = 1e-06
NEGATIVE = -1e30
F32 = jnp.float32
BF16 = jnp.bfloat16

NN = (((1,), (0,)), ((), ()))
NT = (((1,), (1,)), ((), ()))
TN = (((0,), (0,)), ((), ()))


def dot1(a, b, dims=NN):
    return lax.dot_general(a.astype(BF16), b.astype(BF16), dims, preferred_element_type=F32)


def halves(a):
    high = a.astype(BF16)
    return high, (a - high.astype(F32)).astype(BF16)


def dot3(a, b, dims=NN):
    ah, al = halves(a)
    bh, bl = halves(b)
    one = functools.partial(lax.dot_general, dimension_numbers=dims, preferred_element_type=F32)
    return one(ah, bh) + (one(al, bh) + one(ah, bl))


def swapped(place, turn):
    bit = 1
    while bit <= turn:
        if turn & bit:
            place = place + bit - 2 * bit * lax.rem(lax.div(place, bit), 2)
        bit *= 2
    return place


def normalize(pieces, gain, normed, me, here):
    count = len(pieces)
    width = pieces[0].shape[1]
    wides = [piece[here, :].astype(F32) for piece in pieces]
    total = sum(jnp.sum(wide * wide, axis=-1, keepdims=True) for wide in wides)
    scale = lax.rsqrt(total / (width * count) + NORM_EPS)
    for turn, wide in enumerate(wides):
        columns = pl.ds(pl.multiple_of(swapped(me, turn) * width, LANES), width)
        normed[here, columns] = (wide * scale * gain[:, columns]).astype(BF16)


def recurrent_body(group, between, r_ref, k_ref, v_ref, d_ref, learn_ref, out_ref, turn_ref, end_ref, state):
    rows, features = r_ref.shape
    pairs = features // LANES
    lane = lax.broadcasted_iota(jnp.int32, (1, LANES), 1)
    first = (lane < HD).astype(F32)
    second = 1.0 - first
    line = lax.broadcasted_iota(jnp.int32, (LANES, LANES), 0)
    column = lax.broadcasted_iota(jnp.int32, (LANES, LANES), 1)
    strict = line > column
    causal = line >= column
    eye = (line == column).astype(F32)
    same_head = ((line // HD) == (column // HD)).astype(BF16)
    small_line = lax.broadcasted_iota(jnp.int32, (CHUNK, CHUNK), 0)
    small_column = lax.broadcasted_iota(jnp.int32, (CHUNK, CHUNK), 1)
    lower = (small_line >= small_column).astype(BF16)

    def below(size):
        return ((line // size) == (column // size) + 1) & ((line // size) % 2 == 1)

    def spread(x):
        return jnp.concatenate([x * first, x * second], axis=0)

    for pair in range(pairs):
        state[pair, :LANES, :] = jnp.zeros((LANES, LANES), F32)
        state[pair, LANES:, :] = eye

    def local(pair, at):
        here = (pl.ds(at, CHUNK), pl.ds(pair * LANES, LANES))
        r = r_ref[here].astype(F32)
        k = k_ref[here].astype(F32)
        v = v_ref[here].astype(F32)
        decay = d_ref[here]
        learn = learn_ref[:, pl.ds(pair * LANES, LANES)]
        dh = decay.astype(BF16)
        rest = decay - dh.astype(F32)
        dm = rest.astype(BF16)
        dl = (rest - dm.astype(F32)).astype(BF16)
        running = dot1(lower, dh) + (dot1(lower, dm) + dot1(lower, dl))
        before = running - decay
        middle = running[CHUNK // 2 - 1 : CHUNK // 2, :]
        ending = running[CHUNK - 1 :, :]
        sh, sl = halves(k * k)
        squares = dot1(sh, same_head) + dot1(sl, same_head)
        unit = k * lax.rsqrt(squares + KEY_EPS)
        erase = unit * learn
        rise = jnp.exp(middle - running)
        left = jnp.concatenate(
            [spread(-unit * jnp.exp(before - middle)), spread(r * jnp.exp(running - middle))], axis=0
        )
        right = jnp.concatenate([spread(erase * rise), spread(k * rise)], axis=0)
        to_end = jnp.exp(ending - running)
        return dict(
            left=left,
            right=right,
            against=spread(-unit * jnp.exp(before)),
            read=spread(r * jnp.exp(running)),
            erase_end=spread(erase * to_end),
            keys_end=spread(k * to_end),
            values=spread(v),
            whole=jnp.exp(ending),
        )

    def step(turn, carry):
        between(turn)
        spots = [(turn * group + g, pair) for g in range(group) for pair in range(pairs)]
        items = [local(pair, pl.multiple_of(c * CHUNK, CHUNK)) for c, pair in spots]
        for it in items:
            scores = dot1(it["left"], it["right"], NT)
            it["low"] = jnp.where(strict, scores[:LANES, :LANES], 0.0)
            it["carry"] = jnp.where(strict, scores[:LANES, LANES:], 0.0)
            it["read_erase"] = jnp.where(causal, scores[LANES:, :LANES], 0.0)
            it["read_keys"] = jnp.where(causal, scores[LANES:, LANES:], 0.0)
            it["inv"] = eye + jnp.where(below(1), it["low"], 0.0)
        size = 2
        while size < CHUNK:
            keep = below(size)
            for it in items:
                it["mid"] = dot1(jnp.where(keep, it["low"], 0.0), it["inv"])
            for it in items:
                it["inv"] = it["inv"] + dot1(it["inv"], it["mid"])
            size *= 2
        for it in items:
            it["fed"] = dot1(it["carry"], it["values"])
        for it in items:
            side = jnp.concatenate([it["against"], it["fed"]], axis=1)
            it["solved"] = dot1(it["inv"], side)
        for it in items:
            seen = dot1(it["read_erase"], it["solved"])
            it["heard"] = seen[:, LANES:] + dot1(it["read_keys"], it["values"])
            it["read"] = it["read"] + seen[:, :LANES]
            it["added"] = dot1(it["values"], it["keys_end"], TN)
        for (c, pair), it in zip(spots, items):
            now = state[pair]
            both = jnp.concatenate([it["solved"][:, :LANES], it["read"]], axis=0)
            met = dot1(both, now, NT)
            gone = jnp.concatenate(
                [met[:LANES, :LANES] + it["solved"][:, LANES:], met[:LANES, LANES:]], axis=1
            )
            later = now * it["whole"] + dot1(gone, it["erase_end"], TN)
            state[pair, :LANES, :] = later[:LANES] + it["added"]
            state[pair, LANES:, :] = later[LANES:]
            heard = met[LANES:, :LANES] + it["heard"]
            turned = met[LANES:, LANES:]
            here = (pl.ds(pl.multiple_of(c * CHUNK, CHUNK), CHUNK), pl.ds(pair * LANES, LANES))
            out_ref[here] = heard[:CHUNK] + heard[CHUNK:]
            turn_ref[here] = turned[:CHUNK] + turned[CHUNK:]
        return carry

    lax.fori_loop(0, rows // CHUNK // group, step, 0)
    for pair in range(pairs):
        now = state[pair]
        end_ref[pair, :HD, :] = (now[:HD] + now[HD:LANES]).astype(BF16)
        end_ref[pair, HD:, :] = (now[LANES : LANES + HD] + now[LANES + HD :]).astype(BF16)


def join_body(met, own, following, state):
    lane = lax.broadcasted_iota(jnp.int32, (1, LANES), 1)
    first = (lane < HD).astype(F32)
    second = 1.0 - first
    line = lax.broadcasted_iota(jnp.int32, (HD, LANES), 0)
    column = lax.broadcasted_iota(jnp.int32, (HD, LANES), 1)
    eye = (line == lax.rem(column, HD)).astype(F32)

    def spread(x):
        return jnp.concatenate([x * first, x * second], axis=0)

    for pair in range(own.shape[0]):
        both = spread(met[pair, :HD, :].astype(F32))
        if following is not None:
            both = jnp.concatenate([both, spread(met[pair, HD:, :].astype(F32))], axis=0)

        def after(block, size):
            high, low = halves(spread(block[HD : 2 * HD]))
            moved = dot1(both[:size], high) + dot1(both[:size], low)
            return [moved[at : at + HD] + moved[at + HD : at + LANES] for at in range(0, size, LANES)]

        later = state[pair, : 2 * HD, :] + jnp.concatenate([jnp.zeros((HD, LANES), F32), eye], axis=0)
        parts = after(later, 2 * LANES if following is not None else LANES)
        state[pair, :HD, :] = parts[0] + later[:HD]
        if following is not None:
            state[pair, HD : 2 * HD, :] = parts[1] - eye
        if following is not None:
            mine = own[pair].astype(F32)
            parts = after(mine, 2 * LANES)
            following[pair] = jnp.concatenate([parts[0] + mine[:HD], parts[1]], axis=0).astype(BF16)


def finish_body(out_ref, turn_ref, state, mix_ref):
    pairs = out_ref.shape[1] // LANES
    lane = lax.broadcasted_iota(jnp.int32, (1, LANES), 1)
    first = (lane < HD).astype(F32)
    second = 1.0 - first
    line = lax.broadcasted_iota(jnp.int32, (LANES, LANES), 0)
    column = lax.broadcasted_iota(jnp.int32, (LANES, LANES), 1)
    same_head = ((line // HD) == (column // HD)).astype(BF16)

    def spread(x):
        return jnp.concatenate([x * first, x * second], axis=0)

    for pair in range(pairs):
        entering = spread(state[pair, :HD, :])
        columns = pl.ds(pair * LANES, LANES)
        full = out_ref[:, columns] + dot3(turn_ref[:, columns], entering, NT)

        def mean(x):
            high, low = halves(x)
            return (dot1(high, same_head) + dot1(low, same_head)) * (1.0 / HD)

        centered = full - mean(full)
        mix_ref[pair] = (centered * lax.rsqrt(mean(centered * centered) + GROUP_EPS)).astype(
            BF16
        )


def attend(q, kv, head, index, lam, queries, tops, sums, accs, mix_ref, log_ref):
    tiles = queries.shape[0]
    lane = lax.broadcasted_iota(jnp.int32, (1, LANES), 1)
    for tile in range(tiles):
        part = q[pl.ds(tile * LANES, LANES), :].astype(F32) * HD ** (-0.5)
        queries[tile] = jnp.concatenate(
            [jnp.where(lane < HD, part, 0.0), jnp.where(lane < HD, 0.0, part)], axis=0
        ).astype(BF16)
    tops[...] = jnp.full(tops.shape, NEGATIVE, F32)
    sums[...] = jnp.zeros(sums.shape, F32)
    accs[...] = jnp.zeros(accs.shape, F32)

    def score(tile, spots, mask):
        keys = jnp.concatenate([kv[n, head, c, :LANES, :] for n, c in spots], axis=0)
        s = lax.dot_general(keys, queries[tile], NT, preferred_element_type=F32)
        return s if mask is None else jnp.where(mask, s, NEGATIVE)

    def absorb(tile, spots, s):
        values = jnp.concatenate([kv[n, head, c, LANES:, :] for n, c in spots], axis=1)
        old = tops[tile]
        top = jnp.maximum(old, jnp.max(s, axis=0, keepdims=True))
        fade = jnp.exp(old - top)
        weights = jnp.exp(s - top)
        row_sum = sums[tile] * fade + jnp.sum(weights, axis=0, keepdims=True)
        acc = accs[tile] * fade + jnp.dot(
            values, weights.astype(BF16), preferred_element_type=F32
        )
        return top, row_sum, acc

    def fold(numbers):
        spots = [(n, c) for n in numbers for c in range(tiles)]
        scores = {ahead: score(ahead, spots, None) for ahead in range(1)}
        for tile in range(tiles):
            if tile + 1 < tiles:
                scores[tile + 1] = score(tile + 1, spots, None)
            top, row_sum, acc = absorb(tile, spots, scores.pop(tile))
            tops[tile] = top
            sums[tile] = row_sum
            accs[tile] = acc

    def both(turn, carry):
        fold([2 * turn, 2 * turn + 1])
        return carry

    lax.fori_loop(0, lax.div(index, 2), both, 0)
    pl.when(lax.rem(index, 2) == 1)(lambda: fold([index - 1]))
    spots = [(index, c) for c in range(tiles)]
    scores = []
    for tile in range(tiles):
        size = (tile + 1) * LANES
        asking = lax.broadcasted_iota(jnp.int32, (size, LANES), 1) + tile * LANES
        seen = asking >= lax.broadcasted_iota(jnp.int32, (size, LANES), 0)
        mask = jnp.concatenate([seen, seen], axis=1)
        scores.append(score(tile, spots[: tile + 1], mask))
    results = [absorb(tile, spots[: tile + 1], s) for tile, s in enumerate(scores)]
    for tile, (top, row_sum, acc) in enumerate(results):
        maps = acc / row_sum
        logs = top + jnp.log(row_sum)
        here = pl.ds(tile * LANES, LANES)
        log_ref[0:1, here] = logs[:, :LANES]
        log_ref[1:2, here] = logs[:, LANES:]
        out = maps[:, :LANES] - lam * maps[:, LANES:]
        out = out * lax.rsqrt(jnp.mean(out * out, axis=0, keepdims=True) + HEAD_EPS)
        mix_ref[here, :] = jnp.transpose(out).astype(BF16)


def layer_body(sp, tp, *refs):
    (hidden, gain, wr_h, wk_h, wv_h, down_h, up_h, base, shift, learn) = refs[:10]
    (wq_h, wkp_h, wvp_h, lam, rec_h, att_h, out_gain, out, logs) = refs[10:19]
    (xs, normed, wr, wk, wv, down, up, wq, wkp, wvp, hw) = refs[19:30]
    (wb, bmix, wq_p, wkp_p, wvp_p, spare, kv, r, k, v, d, q, heard, turned, ends, met, state) = refs[30:47]
    (queries, top, row_sum, acc, mix, moved, q_far, mix_far, log_far) = refs[47:56]
    (log_got, total, parts, got) = refs[56:60]
    (load, x_send, x_recv, w_send, w_recv, z_send, z_recv, c_send, c_recv) = refs[60:69]
    (e_send, e_recv, q_send, q_recv, b_send, b_recv, m_send, m_recv) = refs[69:77]
    (p_send, p_recv, g_send, l_send, l_recv) = refs[77:]
    rows, features = r.shape
    heads = q.shape[0]
    wide = heads * LANES
    pairs = features // LANES
    me = lax.axis_index("tp")
    place = lax.axis_index("sp")
    count = sp // 2
    level = lax.div(place, 2)
    across = swapped(place, 1)
    mirror = sp - 1 - place
    early = place < count
    late = place >= count
    stay = (heads - heads // 2) * LANES
    moving = list(range(heads - heads // 2, heads))
    staying = list(range(heads - heads // 2))
    parts_of = z_recv.shape[2]
    piece = rows // parts_of

    barrier = pltpu.get_barrier_semaphore()
    for turn in range(1, tp):
        pl.semaphore_signal(barrier, inc=1, device_id={"tp": swapped(me, turn)})
    for hop in range(1, sp):
        pl.semaphore_signal(barrier, inc=1, device_id={"sp": lax.rem(place + hop, sp)})
    for turn in range(1, tp) if moving else ():
        pl.semaphore_signal(barrier, inc=1, device_id={"sp": mirror, "tp": swapped(me, turn)})
    pair_loads = heads > 1
    loads = []
    for number, (source, target) in enumerate(
        (
            (wkp_h, wkp_p if pair_loads else wkp),
            (wvp_h, wvp_p if pair_loads else wvp),
            (wq_h, wq_p if pair_loads else wq),
            (wr_h, wr),
            (wk_h, wk),
            (wv_h, wv),
            (down_h, down),
            (up_h, up),
            (rec_h, hw.at[0, pl.ds(0, features)]),
            (att_h.at[pl.ds(0, stay)], hw.at[0, pl.ds(features, stay)]),
        )
        + (((att_h.at[pl.ds(stay, wide - stay)], wb.at[0]),) if moving else ())
    ):
        loads.append(pltpu.make_async_copy(source, target, load.at[number]))
        loads[-1].start()
    pl.semaphore_wait(barrier, (2 if moving else 1) * (tp - 1) + sp - 1)

    def remote(source, target, send, recv, device):
        return pltpu.make_async_remote_copy(
            src_ref=source, dst_ref=target, send_sem=send, recv_sem=recv, device_id=device
        )

    chunks = [pl.ds(number * piece, piece) for number in range(parts_of)]
    hops = {}
    for turn in range(1, tp):
        for number, here in enumerate(chunks):
            source = hidden if turn < 2 or turn % 2 == 0 else xs.at[turn - 1]
            hops[turn, number] = remote(
                source.at[here],
                xs.at[turn, here],
                x_send.at[turn, number],
                x_recv.at[turn, number],
                {"tp": swapped(me, turn if turn % 2 == 0 else 1)},
            )
    for number in range(parts_of):
        for turn in range(2, tp, 2):
            hops[turn, number].start()
        hops[1, number].start()

    def unpack(packed, target):
        lines = target.shape[0]
        step = lines // 4
        for turn in range(4):
            spare[pl.ds(turn * step * heads, step * heads), :] = packed[
                pl.ds(turn * step * heads, step * heads), :
            ].astype(F32)
        for turn in range(4):
            for head in range(heads):
                target[pl.ds(turn * step, step), pl.ds(head * LANES, LANES)] = spare[
                    pl.ds(turn * step * heads + head, step, stride=heads), :
                ].astype(BF16)

    loads[0].wait()
    loads[1].wait()
    if pair_loads:
        unpack(wkp_p, wkp)
        unpack(wvp_p, wvp)
    loads[2].wait()
    if pair_loads:
        unpack(wq_p, wq)

    def column(head, source, target, number):
        here = kv.at[source, head, number]
        return remote(
            here,
            here,
            z_send.at[head, target, number],
            z_recv.at[head, source_level(source), number],
            {"sp": 2 * target + lax.rem(place, 2)},
        )

    def source_level(source):
        return lax.div(source, 2)

    def crossing(head, source, number):
        here = kv.at[source, head, number]
        return remote(
            here,
            here,
            c_send.at[head, source_level(source), number],
            c_recv.at[head, source_level(source), number],
            {"sp": across},
        )

    def column_goes():
        plan = []
        for target in range(count - 1, -1, -1):
            for head in staying:
                plan.append((head, target, target > level))
            if target < count // 2:
                for head in moving:
                    plan.append((head, target, (target != level) & (level <= count - 1 - target)))
        return plan

    own_crosses = [(head, lax.rem(place, 2) == 0) for head in staying] + [
        (head, level < count // 2) for head in moving
    ]
    relayed = []
    for far in range(1, count):
        for head in staying:
            relayed.append((head, level - far, level >= far))
        for head in moving:
            relayed.append(
                (head, level + far, (level < count // 2) & (level + far <= count - 1 - level))
            )
            relayed.append((head, level - far, (level < count // 2) & (level >= far)))

    def guarded(condition, work):
        pl.when(condition)(work)

    def send_piece(number):
        for head, condition in own_crosses:
            guarded(condition, lambda head=head: crossing(head, place, number).start())
        for head, target, condition in column_goes():
            guarded(
                condition,
                lambda head=head, target=target: column(head, place, target, number).start(),
            )

    def relay(number):
        for head, source, condition in relayed:

            def one(head=head, source=source):
                slot = 2 * source + lax.rem(place, 2)
                column(head, slot, level, number).wait_recv()
                crossing(head, slot, number).start()

            guarded(condition, one)

    def product(here, weight):
        return jnp.dot(normed[here, :], weight[...], preferred_element_type=F32)

    def pass_on(number):
        for turn in range(2, tp, 2):
            hops[turn, number].wait_recv()
            hops[turn + 1, number].start()

    pass_on(0)
    for number, here in enumerate(chunks):
        for turn in range(1, tp, 2):
            hops[turn, number].wait_recv()
        normalize([hidden] + [xs.at[turn] for turn in range(1, tp)], gain, normed, me, here)
        keys = product(here, wkp)
        values = product(here, wvp)
        for head in range(heads):
            columns = slice(head * LANES, (head + 1) * LANES)
            kv[place, head, number, :LANES, :] = keys[:, columns].astype(BF16)
            kv[place, head, number, LANES:, :] = jnp.transpose(values[:, columns]).astype(BF16)
        send_piece(number)
        if number + 1 < parts_of:
            pass_on(number + 1)
        if number == 0:
            for one in loads[3:]:
                one.wait()
            outs = remote(
                hw.at[0], hw.at[1], w_send.at[0], w_recv.at[0], {"tp": swapped(me, 1)}
            )
            outs.start()
        mine = product(here, wq).astype(BF16)
        for head in range(heads):
            q[head, here, :] = mine[:, head * LANES : (head + 1) * LANES]
        r[here, :] = product(here, wr).astype(BF16)
        k[here, :] = product(here, wk).astype(BF16)
        v[here, :] = product(here, wv).astype(BF16)
        low_rank = jnp.tanh(product(here, down)).astype(BF16)
        pre = jnp.dot(low_rank, up[...], preferred_element_type=F32) + base[...]
        d[here, :] = -DECAY_SCALE * jax.nn.sigmoid(pre) + shift[here, :]

    spreads = {}
    for turn in range(1, tp) if moving else ():
        spreads[turn] = remote(
            wb.at[turn - 1] if turn % 2 else wb.at[0],
            wb.at[turn],
            w_send.at[turn],
            w_recv.at[turn],
            {"tp": swapped(me, 1 if turn % 2 else turn)},
        )
    for turn in range(2, tp, 2) if moving else ():
        spreads[turn].start()
    if moving:
        spreads[1].start()

    asks = [
        remote(q.at[head], q_far.at[n], q_send.at[n], q_recv.at[n], {"sp": mirror})
        for n, head in enumerate(moving)
    ]
    if moving:
        guarded(late, lambda: [one.start() for one in asks] and None)

    group = 3 if (rows // CHUNK) % 3 == 0 else 1
    turns = rows // CHUNK // group
    placed = {}
    for number in range(parts_of - 1):
        placed.setdefault(min(number, turns - 1), []).append(number)

    def between(turn):
        for when, numbers in placed.items():

            def work(numbers=numbers):
                for number in numbers:
                    relay(number)

            pl.when(turn == when)(work)

    recurrent_body(group, between, r, k, v, d, learn, heard, turned, ends.at[0], state)
    scans = [1 << number for number in range(ends.shape[0])]
    states = [
        remote(
            ends.at[number, :, pl.ds(0, HD if number + 1 == len(scans) else 2 * HD)],
            met.at[number, :, pl.ds(0, HD if number + 1 == len(scans) else 2 * HD)],
            e_send.at[number],
            e_recv.at[number],
            {"sp": place + hop},
        )
        for number, hop in enumerate(scans)
    ]
    guarded(place + 1 < sp, states[0].start)

    def scan(number):
        hop = scans[number]
        last = number + 1 == len(scans)

        def take():
            states[number].wait_recv()
            join_body(met.at[number], ends.at[number], None if last else ends.at[number + 1], state)

        guarded(place >= hop, take)
        if not last:

            def keep():
                ends[number + 1] = ends[number]

            guarded(place < hop, keep)
            guarded(place + 2 * hop < sp, states[number + 1].start)

    relay(parts_of - 1)

    def arrive(names, last):
        for source in range(count):
            for side in range(2):
                slot = 2 * source + side

                def one(slot=slot):
                    for head in names:
                        for number in range(parts_of):
                            crossing(head, slot, number).wait_recv()

                guarded((lax.rem(place, 2) != side) & (slot <= last), one)

    part = rows // tp
    mate = swapped(me, 1)

    def lines(owner):
        return pl.ds(pl.multiple_of(owner * part, part), part)

    answers, gives, tells = [], [], []
    if moving:
        for turn in range(tp):
            owner = swapped(me, turn)
            answers.append(
                remote(
                    mix_far.at[:, lines(owner)],
                    bmix.at[turn],
                    b_send.at[turn],
                    b_recv.at[turn],
                    {"sp": mirror, "tp": owner} if turn else {"sp": mirror},
                )
            )
            if turn:
                gives.append(
                    remote(
                        mix.at[pl.ds(pairs + moving[0], len(moving)), lines(owner)],
                        bmix.at[turn],
                        g_send.at[turn],
                        b_recv.at[turn],
                        {"tp": owner},
                    )
                )
        tells.append(
            remote(log_far, log_got, l_send.at[0], l_recv.at[0], {"sp": mirror})
        )
    work = (queries, top, row_sum, acc)

    state[...] = jnp.zeros(state.shape, F32)
    scan(0)
    arrive(staying, place)
    for head in staying:
        attend(
            q.at[head], kv, head, place, lam[head], *work, mix.at[pairs + head], logs.at[head]
        )
    for number in range(1, len(scans) - 1):
        scan(number)
    if len(scans) > 1:
        scan(len(scans) - 1)
    finish_body(heard, turned, state, mix)
    blocks = pairs + len(staying)
    swaps = []
    for turn in range(tp // 2):
        theirs = lines(lax.rem(mate + 2 * turn, tp))
        swaps.append(
            remote(
                mix.at[pl.ds(0, blocks), theirs],
                moved.at[:, theirs],
                m_send.at[turn],
                m_recv.at[turn],
                {"tp": mate},
            )
        )
    for one in swaps:
        one.start()
    owners = [lax.rem(me + 2 * turn, tp) for turn in range(1, tp // 2)] + [me]
    outs.wait_recv()
    for one in swaps:
        one.wait_recv()
    near = jnp.concatenate(
        [
            jnp.concatenate([mix[b, lines(owner), :] for b in range(blocks)], axis=1)
            for owner in owners
        ],
        axis=0,
    )
    far = jnp.concatenate(
        [
            jnp.concatenate([moved[b, lines(owner), :] for b in range(blocks)], axis=1)
            for owner in owners
        ],
        axis=0,
    )
    slabs, slab = parts.shape[1], parts.shape[3]
    trades = {}
    for number in range(slabs):
        columns = pl.ds(number * slab, slab)
        result = jnp.dot(near, hw[0, :, columns], preferred_element_type=F32)
        result = result + jnp.dot(far, hw[1, :, columns], preferred_element_type=F32)
        for turn in range(1, tp // 2):
            parts[turn, number] = result[(turn - 1) * part : turn * part].astype(BF16)
            trades[turn, number] = remote(
                parts.at[turn, number],
                got.at[turn, number],
                p_send.at[turn, number],
                p_recv.at[turn, number],
                {"tp": lax.rem(me + 2 * turn, tp)},
            )
            trades[turn, number].start()
        total[:, columns] = result[(tp // 2 - 1) * part :]
    if moving:
        spreads[1].wait_recv()
        for turn in range(2, tp, 2):
            spreads[turn].wait_recv()
            spreads[turn + 1].start()
    if moving:

        def foreign():
            arrive(moving, mirror)
            for n, head in enumerate(moving):
                asks[n].wait_recv()
                attend(
                    q_far.at[n], kv, head, mirror, lam[head], *work, mix_far.at[n], log_far.at[n]
                )
            for one in answers + tells:
                one.start()

        guarded(early, foreign)
    if moving:

        def local():
            for head in moving:
                attend(
                    q.at[head],
                    kv,
                    head,
                    place,
                    lam[head],
                    *work,
                    mix.at[pairs + head],
                    logs.at[head],
                )
            for one in gives:
                one.start()
            for n, head in enumerate(moving):
                bmix[0, n] = mix[pairs + head, lines(me), :]
            for one in gives:
                one.wait_recv()

        def collect():
            for one in answers + tells:
                one.wait_recv()
            for n, head in enumerate(moving):
                logs[head] = log_got[n]

        guarded(early, local)
        guarded(late, collect)
    if moving:
        for turn in range(3, tp, 2):
            spreads[turn].wait_recv()
        beside = jnp.concatenate(
            [bmix[turn, n] for turn in range(tp) for n in range(len(moving))], axis=1
        )
    for number in range(slabs):
        columns = pl.ds(number * slab, slab)
        full = total[:, columns]
        if moving:
            weights = jnp.concatenate([wb[turn, :, columns] for turn in range(tp)], axis=0)
            full = full + jnp.dot(beside, weights, preferred_element_type=F32)
        for turn in range(1, tp // 2):
            trades[turn, number].wait_recv()
            full = full + got[turn, number].astype(F32)
        total[:, columns] = full
    full = total[...]
    mean = jnp.mean(full * full, axis=-1, keepdims=True)
    out[...] = (full * lax.rsqrt(mean + NORM_EPS) * out_gain[...]).astype(BF16)

    for group_of in (hops, trades, spreads):
        for one in group_of.values():
            one.wait_send()
    for one in swaps:
        one.wait_send()
    outs.wait_send()
    for number in range(parts_of):
        for head, condition in own_crosses:
            guarded(condition, crossing(head, place, number).wait_send)
        for head, target, condition in column_goes():
            guarded(condition, column(head, place, target, number).wait_send)
    for head, source, condition in relayed:

        def one(head=head, source=source):
            for number in range(parts_of):
                slot = 2 * source + lax.rem(place, 2)
                crossing(head, slot, number).wait_send()

        guarded(condition, one)
    for number, hop in enumerate(scans):
        guarded(place + hop < sp, states[number].wait_send)
    if moving:
        guarded(late, lambda: [one.wait_send() for one in asks] and None)
        guarded(early, lambda: [one.wait_send() for one in answers + gives + tells] and None)


def per_device(
    sp,
    tp,
    hidden_in,
    in_gain,
    receptance_weight,
    key_weight,
    value_weight,
    decay_down,
    decay_up,
    decay_base,
    decay_shift,
    learn_rate,
    query_pair,
    key_pair,
    value_pair,
    mix_lambda,
    out_recurrent,
    out_attention,
    out_gain,
):
    rows, width = hidden_in.shape
    depth = width * tp
    features = receptance_weight.shape[1]
    heads = mix_lambda.shape[0]
    wide = heads * LANES
    pairs = features // LANES
    low = decay_down.shape[1]
    across = out_recurrent.shape[1]
    part = rows // tp
    count = sp // 2
    movers = max(heads // 2, 1)
    stay = (heads - heads // 2) * LANES
    gone = max(wide - stay, 16)
    pieces = rows // LANES
    slabs = 4 if across % (4 * LANES) == 0 else 1
    shape = jax.ShapeDtypeStruct
    held = pltpu.VMEM

    def paired(weight):
        return weight.reshape(depth * heads, LANES)

    args = (
        hidden_in,
        in_gain.reshape(1, -1),
        receptance_weight,
        key_weight,
        value_weight,
        decay_down,
        decay_up,
        decay_base.reshape(1, -1),
        decay_shift,
        learn_rate.reshape(1, -1),
        paired(query_pair),
        paired(key_pair),
        paired(value_pair),
        mix_lambda,
        out_recurrent,
        out_attention,
        out_gain.reshape(1, -1),
    )
    inside = pl.BlockSpec(memory_space=pltpu.VMEM)
    outside = pl.BlockSpec(memory_space=pl.ANY)
    specs = [inside] * 2 + [outside] * 5 + [inside] * 3 + [outside] * 3
    specs += [pl.BlockSpec(memory_space=pltpu.SMEM)] + [outside] * 2 + [inside]
    raw = (depth * heads, LANES) if heads > 1 else (16, LANES)
    scans = max((sp - 1).bit_length(), 1)
    sizes = ((11,), (tp, pieces), (tp, pieces), (tp,), (tp,))
    sizes += ((heads, count, pieces),) * 4
    sizes += ((scans,), (scans,), (movers,), (movers,), (tp,), (tp,))
    sizes += ((tp // 2,), (tp // 2,), (tp // 2, slabs), (tp // 2, slabs))
    sizes += ((tp,), (1,), (1,))
    return tuple(
        pl.pallas_call(
            functools.partial(layer_body, sp, tp),
            out_shape=[shape((part, across), BF16), shape((heads, 2, rows), F32)],
            in_specs=specs,
            out_specs=[inside] * 2,
            scratch_shapes=[
                held((tp, rows, width), BF16),
                held((rows, depth), BF16),
                held((depth, features), BF16),
                held((depth, features), BF16),
                held((depth, features), BF16),
                held((depth, low), BF16),
                held((low, features), BF16),
                held((depth, wide), BF16),
                held((depth, wide), BF16),
                held((depth, wide), BF16),
                held((2, features + stay, across), BF16),
                held((tp, gone, across), BF16),
                held((tp, movers, part, LANES), BF16),
                held(raw, BF16),
                held(raw, BF16),
                held(raw, BF16),
                held(raw, F32),
                held((sp, heads, pieces, 2 * LANES, LANES), BF16),
                held((rows, features), BF16),
                held((rows, features), BF16),
                held((rows, features), BF16),
                held((rows, features), F32),
                held((heads, rows, LANES), BF16),
                held((rows, features), F32),
                held((rows, features), F32),
                held((scans, pairs, 2 * HD, LANES), BF16),
                held((scans, pairs, 2 * HD, LANES), BF16),
                held((pairs, 2 * LANES, LANES), F32),
                held((pieces, 2 * LANES, LANES), BF16),
                held((pieces, 1, 2 * LANES), F32),
                held((pieces, 1, 2 * LANES), F32),
                held((pieces, LANES, 2 * LANES), F32),
                held((pairs + heads, rows, LANES), BF16),
                held((pairs + heads - heads // 2, rows, LANES), BF16),
                held((movers, rows, LANES), BF16),
                held((movers, rows, LANES), BF16),
                held((movers, 2, rows), F32),
                held((movers, 2, rows), F32),
                held((part, across), F32),
                held((tp // 2, slabs, part, across // slabs), BF16),
                held((tp // 2, slabs, part, across // slabs), BF16),
            ]
            + [pltpu.SemaphoreType.DMA(size) for size in sizes],
            compiler_params=pltpu.CompilerParams(
                collective_id=0, has_side_effects=True, vmem_limit_bytes=62 * 1024 * 1024
            ),
        )(*args)
    )


def solution(mesh):
    in_specs = (
        P("sp", "tp"),
        P(),
        P(None, "tp"),
        P(None, "tp"),
        P(None, "tp"),
        P(),
        P(None, "tp"),
        P("tp"),
        P("sp", "tp"),
        P("tp"),
        P(None, "tp", None),
        P(None, "tp", None),
        P(None, "tp", None),
        P("tp"),
        P("tp", None),
        P("tp", None),
        P(),
    )
    out_specs = (P(("sp", "tp"), None), P("tp", None, "sp"))
    body = functools.partial(per_device, mesh.shape["sp"], mesh.shape["tp"])
    return jax.shard_map(
        body, mesh=mesh, in_specs=in_specs, out_specs=out_specs, check_vma=False
    )
```

```python
import functools
import math

import jax
import jax.numpy as jnp
from jax import lax
from jax.experimental import pallas as pl
from jax.experimental.pallas import tpu as pltpu
from jax.sharding import PartitionSpec as P

HD = 64
LANES = 128
CHUNK = 64
DECAY_SCALE = math.exp(-0.5)
NORM_EPS = 1e-06
GROUP_EPS = 0.00064
HEAD_EPS = 1e-05
KEY_EPS = 1e-06
NEGATIVE = -1e30
F32 = jnp.float32
BF16 = jnp.bfloat16

NN = (((1,), (0,)), ((), ()))
NT = (((1,), (1,)), ((), ()))
TN = (((0,), (0,)), ((), ()))


def dot1(a, b, dims=NN):
    return lax.dot_general(a.astype(BF16), b.astype(BF16), dims, preferred_element_type=F32)


def halves(a):
    high = a.astype(BF16)
    return high, (a - high.astype(F32)).astype(BF16)


def dot3(a, b, dims=NN):
    ah, al = halves(a)
    bh, bl = halves(b)
    one = functools.partial(lax.dot_general, dimension_numbers=dims, preferred_element_type=F32)
    return one(ah, bh) + (one(al, bh) + one(ah, bl))


def swapped(place, turn):
    bit = 1
    while bit <= turn:
        if turn & bit:
            place = place + bit - 2 * bit * lax.rem(lax.div(place, bit), 2)
        bit *= 2
    return place


def normalize(pieces, gain, normed, me, here):
    count = len(pieces)
    width = pieces[0].shape[1]
    wides = [piece[here, :].astype(F32) for piece in pieces]
    total = sum(jnp.sum(wide * wide, axis=-1, keepdims=True) for wide in wides)
    scale = lax.rsqrt(total / (width * count) + NORM_EPS)
    for turn, wide in enumerate(wides):
        columns = pl.ds(pl.multiple_of(swapped(me, turn) * width, LANES), width)
        normed[here, columns] = (wide * scale * gain[:, columns]).astype(BF16)


def recurrent_body(group, between, r_ref, k_ref, v_ref, d_ref, learn_ref, out_ref, turn_ref, end_ref, state):
    rows, features = r_ref.shape
    pairs = features // LANES
    lane = lax.broadcasted_iota(jnp.int32, (1, LANES), 1)
    first = (lane < HD).astype(F32)
    second = 1.0 - first
    line = lax.broadcasted_iota(jnp.int32, (LANES, LANES), 0)
    column = lax.broadcasted_iota(jnp.int32, (LANES, LANES), 1)
    strict = line > column
    causal = line >= column
    eye = (line == column).astype(F32)
    same_head = ((line // HD) == (column // HD)).astype(BF16)
    small_line = lax.broadcasted_iota(jnp.int32, (CHUNK, CHUNK), 0)
    small_column = lax.broadcasted_iota(jnp.int32, (CHUNK, CHUNK), 1)
    lower = (small_line >= small_column).astype(BF16)

    def below(size):
        return ((line // size) == (column // size) + 1) & ((line // size) % 2 == 1)

    def spread(x):
        return jnp.concatenate([x * first, x * second], axis=0)

    for pair in range(pairs):
        state[pair, :LANES, :] = jnp.zeros((LANES, LANES), F32)
        state[pair, LANES:, :] = eye

    def local(pair, at):
        here = (pl.ds(at, CHUNK), pl.ds(pair * LANES, LANES))
        r = r_ref[here].astype(F32)
        k = k_ref[here].astype(F32)
        v = v_ref[here].astype(F32)
        decay = d_ref[here]
        learn = learn_ref[:, pl.ds(pair * LANES, LANES)]
        dh = decay.astype(BF16)
        rest = decay - dh.astype(F32)
        dm = rest.astype(BF16)
        dl = (rest - dm.astype(F32)).astype(BF16)
        running = dot1(lower, dh) + (dot1(lower, dm) + dot1(lower, dl))
        before = running - decay
        middle = running[CHUNK // 2 - 1 : CHUNK // 2, :]
        ending = running[CHUNK - 1 :, :]
        sh, sl = halves(k * k)
        squares = dot1(sh, same_head) + dot1(sl, same_head)
        unit = k * lax.rsqrt(squares + KEY_EPS)
        erase = unit * learn
        rise = jnp.exp(middle - running)
        left = jnp.concatenate(
            [spread(-unit * jnp.exp(before - middle)), spread(r * jnp.exp(running - middle))], axis=0
        )
        right = jnp.concatenate([spread(erase * rise), spread(k * rise)], axis=0)
        to_end = jnp.exp(ending - running)
        return dict(
            left=left,
            right=right,
            against=spread(-unit * jnp.exp(before)),
            read=spread(r * jnp.exp(running)),
            erase_end=spread(erase * to_end),
            keys_end=spread(k * to_end),
            values=spread(v),
            whole=jnp.exp(ending),
        )

    def step(turn, carry):
        between(turn)
        spots = [(turn * group + g, pair) for g in range(group) for pair in range(pairs)]
        items = [local(pair, pl.multiple_of(c * CHUNK, CHUNK)) for c, pair in spots]
        for it in items:
            scores = dot1(it["left"], it["right"], NT)
            it["low"] = jnp.where(strict, scores[:LANES, :LANES], 0.0)
            it["carry"] = jnp.where(strict, scores[:LANES, LANES:], 0.0)
            it["read_erase"] = jnp.where(causal, scores[LANES:, :LANES], 0.0)
            it["read_keys"] = jnp.where(causal, scores[LANES:, LANES:], 0.0)
            it["inv"] = eye + jnp.where(below(1), it["low"], 0.0)
        size = 2
        while size < CHUNK:
            keep = below(size)
            for it in items:
                it["mid"] = dot1(jnp.where(keep, it["low"], 0.0), it["inv"])
            for it in items:
                it["inv"] = it["inv"] + dot1(it["inv"], it["mid"])
            size *= 2
        for it in items:
            it["fed"] = dot1(it["carry"], it["values"])
        for it in items:
            side = jnp.concatenate([it["against"], it["fed"]], axis=1)
            it["solved"] = dot1(it["inv"], side)
        for it in items:
            seen = dot1(it["read_erase"], it["solved"])
            it["heard"] = seen[:, LANES:] + dot1(it["read_keys"], it["values"])
            it["read"] = it["read"] + seen[:, :LANES]
            it["added"] = dot1(it["values"], it["keys_end"], TN)
        for (c, pair), it in zip(spots, items):
            now = state[pair]
            both = jnp.concatenate([it["solved"][:, :LANES], it["read"]], axis=0)
            met = dot1(both, now, NT)
            gone = jnp.concatenate(
                [met[:LANES, :LANES] + it["solved"][:, LANES:], met[:LANES, LANES:]], axis=1
            )
            later = now * it["whole"] + dot1(gone, it["erase_end"], TN)
            state[pair, :LANES, :] = later[:LANES] + it["added"]
            state[pair, LANES:, :] = later[LANES:]
            heard = met[LANES:, :LANES] + it["heard"]
            turned = met[LANES:, LANES:]
            here = (pl.ds(pl.multiple_of(c * CHUNK, CHUNK), CHUNK), pl.ds(pair * LANES, LANES))
            out_ref[here] = heard[:CHUNK] + heard[CHUNK:]
            turn_ref[here] = turned[:CHUNK] + turned[CHUNK:]
        return carry

    lax.fori_loop(0, rows // CHUNK // group, step, 0)
    for pair in range(pairs):
        now = state[pair]
        end_ref[pair, :HD, :] = (now[:HD] + now[HD:LANES]).astype(BF16)
        end_ref[pair, HD:, :] = (now[LANES : LANES + HD] + now[LANES + HD :]).astype(BF16)


def join_body(met, own, following, state):
    lane = lax.broadcasted_iota(jnp.int32, (1, LANES), 1)
    first = (lane < HD).astype(F32)
    second = 1.0 - first
    line = lax.broadcasted_iota(jnp.int32, (HD, LANES), 0)
    column = lax.broadcasted_iota(jnp.int32, (HD, LANES), 1)
    eye = (line == lax.rem(column, HD)).astype(F32)

    def spread(x):
        return jnp.concatenate([x * first, x * second], axis=0)

    for pair in range(own.shape[0]):
        both = spread(met[pair, :HD, :].astype(F32))
        if following is not None:
            both = jnp.concatenate([both, spread(met[pair, HD:, :].astype(F32))], axis=0)

        def after(block, size):
            high, low = halves(spread(block[HD : 2 * HD]))
            moved = dot1(both[:size], high) + dot1(both[:size], low)
            return [moved[at : at + HD] + moved[at + HD : at + LANES] for at in range(0, size, LANES)]

        later = state[pair, : 2 * HD, :] + jnp.concatenate([jnp.zeros((HD, LANES), F32), eye], axis=0)
        parts = after(later, 2 * LANES if following is not None else LANES)
        state[pair, :HD, :] = parts[0] + later[:HD]
        if following is not None:
            state[pair, HD : 2 * HD, :] = parts[1] - eye
        if following is not None:
            mine = own[pair].astype(F32)
            parts = after(mine, 2 * LANES)
            following[pair] = jnp.concatenate([parts[0] + mine[:HD], parts[1]], axis=0).astype(BF16)


def finish_body(out_ref, turn_ref, state, mix_ref):
    pairs = out_ref.shape[1] // LANES
    lane = lax.broadcasted_iota(jnp.int32, (1, LANES), 1)
    first = (lane < HD).astype(F32)
    second = 1.0 - first
    line = lax.broadcasted_iota(jnp.int32, (LANES, LANES), 0)
    column = lax.broadcasted_iota(jnp.int32, (LANES, LANES), 1)
    same_head = ((line // HD) == (column // HD)).astype(BF16)

    def spread(x):
        return jnp.concatenate([x * first, x * second], axis=0)

    for pair in range(pairs):
        entering = spread(state[pair, :HD, :])
        columns = pl.ds(pair * LANES, LANES)
        full = out_ref[:, columns] + dot3(turn_ref[:, columns], entering, NT)

        def mean(x):
            high, low = halves(x)
            return (dot1(high, same_head) + dot1(low, same_head)) * (1.0 / HD)

        centered = full - mean(full)
        mix_ref[pair] = (centered * lax.rsqrt(mean(centered * centered) + GROUP_EPS)).astype(
            BF16
        )


def attend(q, kv, head, index, lam, queries, tops, sums, accs, mix_ref, log_ref):
    tiles = queries.shape[0]
    lane = lax.broadcasted_iota(jnp.int32, (1, LANES), 1)
    for tile in range(tiles):
        part = q[pl.ds(tile * LANES, LANES), :].astype(F32) * HD ** (-0.5)
        queries[tile] = jnp.concatenate(
            [jnp.where(lane < HD, part, 0.0), jnp.where(lane < HD, 0.0, part)], axis=0
        ).astype(BF16)
    tops[...] = jnp.full(tops.shape, NEGATIVE, F32)
    sums[...] = jnp.zeros(sums.shape, F32)
    accs[...] = jnp.zeros(accs.shape, F32)

    def score(tile, spots, mask):
        keys = jnp.concatenate([kv[n, head, c, :LANES, :] for n, c in spots], axis=0)
        s = lax.dot_general(keys, queries[tile], NT, preferred_element_type=F32)
        return s if mask is None else jnp.where(mask, s, NEGATIVE)

    def absorb(tile, spots, s):
        values = jnp.concatenate([kv[n, head, c, LANES:, :] for n, c in spots], axis=1)
        old = tops[tile]
        top = jnp.maximum(old, jnp.max(s, axis=0, keepdims=True))
        fade = jnp.exp(old - top)
        weights = jnp.exp(s - top)
        row_sum = sums[tile] * fade + jnp.sum(weights, axis=0, keepdims=True)
        acc = accs[tile] * fade + jnp.dot(
            values, weights.astype(BF16), preferred_element_type=F32
        )
        return top, row_sum, acc

    def fold(numbers):
        spots = [(n, c) for n in numbers for c in range(tiles)]
        scores = {ahead: score(ahead, spots, None) for ahead in range(1)}
        for tile in range(tiles):
            if tile + 1 < tiles:
                scores[tile + 1] = score(tile + 1, spots, None)
            top, row_sum, acc = absorb(tile, spots, scores.pop(tile))
            tops[tile] = top
            sums[tile] = row_sum
            accs[tile] = acc

    def both(turn, carry):
        fold([2 * turn, 2 * turn + 1])
        return carry

    lax.fori_loop(0, lax.div(index, 2), both, 0)
    pl.when(lax.rem(index, 2) == 1)(lambda: fold([index - 1]))
    spots = [(index, c) for c in range(tiles)]
    scores = []
    for tile in range(tiles):
        size = (tile + 1) * LANES
        asking = lax.broadcasted_iota(jnp.int32, (size, LANES), 1) + tile * LANES
        seen = asking >= lax.broadcasted_iota(jnp.int32, (size, LANES), 0)
        mask = jnp.concatenate([seen, seen], axis=1)
        scores.append(score(tile, spots[: tile + 1], mask))
    results = [absorb(tile, spots[: tile + 1], s) for tile, s in enumerate(scores)]
    for tile, (top, row_sum, acc) in enumerate(results):
        maps = acc / row_sum
        logs = top + jnp.log(row_sum)
        here = pl.ds(tile * LANES, LANES)
        log_ref[0:1, here] = logs[:, :LANES]
        log_ref[1:2, here] = logs[:, LANES:]
        out = maps[:, :LANES] - lam * maps[:, LANES:]
        out = out * lax.rsqrt(jnp.mean(out * out, axis=0, keepdims=True) + HEAD_EPS)
        mix_ref[here, :] = jnp.transpose(out).astype(BF16)


def settle_body(first, second, out, logs, done):
    moves = [
        pltpu.make_async_copy(first, out, done.at[0]),
        pltpu.make_async_copy(second, logs, done.at[1]),
    ]
    for one in moves:
        one.start()
    for one in moves:
        one.wait()


def layer_body(sp, tp, *refs):
    (hidden, gain, wr_h, wk_h, wv_h, down_h, up_h, base, shift, learn) = refs[:10]
    (wq_h, wkp_h, wvp_h, lam, rec_h, att_h, out_gain, out, logs) = refs[10:19]
    (xs, normed, wr, wk, wv, down, up, wq, wkp, wvp, hw) = refs[19:30]
    (wb, bmix, wq_p, wkp_p, wvp_p, spare, kv, r, k, v, d, q, heard, turned, ends, met, state) = refs[30:47]
    (queries, top, row_sum, acc, mix, moved, q_far, mix_far, log_far) = refs[47:56]
    (log_got, total, parts, got) = refs[56:60]
    (load, x_send, x_recv, w_send, w_recv, z_send, z_recv, c_send, c_recv) = refs[60:69]
    (e_send, e_recv, q_send, q_recv, b_send, b_recv, m_send, m_recv) = refs[69:77]
    (p_send, p_recv, g_send, l_send, l_recv) = refs[77:]
    rows, features = r.shape
    heads = q.shape[0]
    wide = heads * LANES
    pairs = features // LANES
    me = lax.axis_index("tp")
    place = lax.axis_index("sp")
    count = sp // 2
    level = lax.div(place, 2)
    across = swapped(place, 1)
    mirror = sp - 1 - place
    early = place < count
    late = place >= count
    stay = (heads - heads // 2) * LANES
    moving = list(range(heads - heads // 2, heads))
    staying = list(range(heads - heads // 2))
    parts_of = z_recv.shape[2]
    piece = rows // parts_of

    barrier = pltpu.get_barrier_semaphore()
    for turn in range(1, tp):
        pl.semaphore_signal(barrier, inc=1, device_id={"tp": swapped(me, turn)})
    for hop in range(1, sp):
        pl.semaphore_signal(barrier, inc=1, device_id={"sp": lax.rem(place + hop, sp)})
    for turn in range(1, tp) if moving else ():
        pl.semaphore_signal(barrier, inc=1, device_id={"sp": mirror, "tp": swapped(me, turn)})
    pair_loads = heads > 1
    loads = []
    for number, (source, target) in enumerate(
        (
            (wkp_h, wkp_p if pair_loads else wkp),
            (wvp_h, wvp_p if pair_loads else wvp),
            (wq_h, wq_p if pair_loads else wq),
            (wr_h, wr),
            (wk_h, wk),
            (wv_h, wv),
            (down_h, down),
            (up_h, up),
            (rec_h, hw.at[0, pl.ds(0, features)]),
            (att_h.at[pl.ds(0, stay)], hw.at[0, pl.ds(features, stay)]),
        )
        + (((att_h.at[pl.ds(stay, wide - stay)], wb.at[0]),) if moving else ())
    ):
        loads.append(pltpu.make_async_copy(source, target, load.at[number]))
        loads[-1].start()
    pl.semaphore_wait(barrier, (2 if moving else 1) * (tp - 1) + sp - 1)

    def remote(source, target, send, recv, device):
        return pltpu.make_async_remote_copy(
            src_ref=source, dst_ref=target, send_sem=send, recv_sem=recv, device_id=device
        )

    chunks = [pl.ds(number * piece, piece) for number in range(parts_of)]
    hops = {}
    for turn in range(1, tp):
        for number, here in enumerate(chunks):
            source = hidden if turn < 2 or turn % 2 == 0 else xs.at[turn - 1]
            hops[turn, number] = remote(
                source.at[here],
                xs.at[turn, here],
                x_send.at[turn, number],
                x_recv.at[turn, number],
                {"tp": swapped(me, turn if turn % 2 == 0 else 1)},
            )
    for number in range(parts_of):
        for turn in range(2, tp, 2):
            hops[turn, number].start()
        hops[1, number].start()

    def unpack(packed, target):
        lines = target.shape[0]
        step = lines // 4
        for turn in range(4):
            spare[pl.ds(turn * step * heads, step * heads), :] = packed[
                pl.ds(turn * step * heads, step * heads), :
            ].astype(F32)
        for turn in range(4):
            for head in range(heads):
                target[pl.ds(turn * step, step), pl.ds(head * LANES, LANES)] = spare[
                    pl.ds(turn * step * heads + head, step, stride=heads), :
                ].astype(BF16)

    loads[0].wait()
    loads[1].wait()
    if pair_loads:
        unpack(wkp_p, wkp)
        unpack(wvp_p, wvp)
    loads[2].wait()
    if pair_loads:
        unpack(wq_p, wq)

    def column(head, source, target, number):
        here = kv.at[source, head, number]
        return remote(
            here,
            here,
            z_send.at[head, target, number],
            z_recv.at[head, source_level(source), number],
            {"sp": 2 * target + lax.rem(place, 2)},
        )

    def source_level(source):
        return lax.div(source, 2)

    def crossing(head, source, number):
        here = kv.at[source, head, number]
        return remote(
            here,
            here,
            c_send.at[head, source_level(source), number],
            c_recv.at[head, source_level(source), number],
            {"sp": across},
        )

    def column_goes():
        plan = []
        for target in range(count - 1, -1, -1):
            for head in staying:
                plan.append((head, target, target > level))
            if target < count // 2:
                for head in moving:
                    plan.append((head, target, (target != level) & (level <= count - 1 - target)))
        return plan

    own_crosses = [(head, lax.rem(place, 2) == 0) for head in staying] + [
        (head, level < count // 2) for head in moving
    ]
    relayed = []
    for far in range(1, count):
        for head in staying:
            relayed.append((head, level - far, level >= far))
        for head in moving:
            relayed.append(
                (head, level + far, (level < count // 2) & (level + far <= count - 1 - level))
            )
            relayed.append((head, level - far, (level < count // 2) & (level >= far)))

    def guarded(condition, work):
        pl.when(condition)(work)

    def send_piece(number):
        for head, condition in own_crosses:
            guarded(condition, lambda head=head: crossing(head, place, number).start())
        for head, target, condition in column_goes():
            guarded(
                condition,
                lambda head=head, target=target: column(head, place, target, number).start(),
            )

    def relay(number, also=None):
        for head, source, condition in relayed:

            def one(head=head, source=source):
                slot = 2 * source + lax.rem(place, 2)
                column(head, slot, level, number).wait_recv()
                crossing(head, slot, number).start()

            guarded(condition if also is None else condition & also, one)

    def product(here, weight):
        return jnp.dot(normed[here, :], weight[...], preferred_element_type=F32)

    def pass_on(number):
        for turn in range(2, tp, 2):
            hops[turn, number].wait_recv()
            hops[turn + 1, number].start()

    pass_on(0)
    for number, here in enumerate(chunks):
        for turn in range(1, tp, 2):
            hops[turn, number].wait_recv()
        normalize([hidden] + [xs.at[turn] for turn in range(1, tp)], gain, normed, me, here)
        keys = product(here, wkp)
        values = product(here, wvp)
        for head in range(heads):
            columns = slice(head * LANES, (head + 1) * LANES)
            kv[place, head, number, :LANES, :] = keys[:, columns].astype(BF16)
            kv[place, head, number, LANES:, :] = jnp.transpose(values[:, columns]).astype(BF16)
        send_piece(number)
        if number + 1 < parts_of:
            pass_on(number + 1)
        if number == 0:
            for one in loads[3:]:
                one.wait()
            outs = remote(
                hw.at[0], hw.at[1], w_send.at[0], w_recv.at[0], {"tp": swapped(me, 1)}
            )
            outs.start()
        mine = product(here, wq).astype(BF16)
        for head in range(heads):
            q[head, here, :] = mine[:, head * LANES : (head + 1) * LANES]
        r[here, :] = product(here, wr).astype(BF16)
        k[here, :] = product(here, wk).astype(BF16)
        v[here, :] = product(here, wv).astype(BF16)
        low_rank = jnp.tanh(product(here, down)).astype(BF16)
        pre = jnp.dot(low_rank, up[...], preferred_element_type=F32) + base[...]
        d[here, :] = -DECAY_SCALE * jax.nn.sigmoid(pre) + shift[here, :]

    spreads = {}
    for turn in range(1, tp) if moving else ():
        spreads[turn] = remote(
            wb.at[turn - 1] if turn % 2 else wb.at[0],
            wb.at[turn],
            w_send.at[turn],
            w_recv.at[turn],
            {"tp": swapped(me, 1 if turn % 2 else turn)},
        )
    for turn in range(2, tp, 2) if moving else ():
        spreads[turn].start()
    if moving:
        spreads[1].start()

    asks = [
        remote(q.at[head], q_far.at[n], q_send.at[n], q_recv.at[n], {"sp": mirror})
        for n, head in enumerate(moving)
    ]
    if moving:
        guarded(late, lambda: [one.start() for one in asks] and None)

    group = 3 if (rows // CHUNK) % 3 == 0 else 1
    turns = rows // CHUNK // group
    placed = {}
    highest = level == count - 1
    for number in range(parts_of - 1):
        placed.setdefault(min(number, turns - 1), []).append(number)

    def between(turn):
        for when, numbers in placed.items():

            def work(numbers=numbers):
                for number in numbers:
                    relay(number, highest if number else None)

            pl.when(turn == when)(work)

    recurrent_body(group, between, r, k, v, d, learn, heard, turned, ends.at[0], state)
    scans = [1 << number for number in range(ends.shape[0])]
    states = [
        remote(
            ends.at[number, :, pl.ds(0, HD if number + 1 == len(scans) else 2 * HD)],
            met.at[number, :, pl.ds(0, HD if number + 1 == len(scans) else 2 * HD)],
            e_send.at[number],
            e_recv.at[number],
            {"sp": place + hop},
        )
        for number, hop in enumerate(scans)
    ]
    guarded(place + 1 < sp, states[0].start)

    def scan(number):
        hop = scans[number]
        last = number + 1 == len(scans)

        def take():
            states[number].wait_recv()
            join_body(met.at[number], ends.at[number], None if last else ends.at[number + 1], state)

        guarded(place >= hop, take)
        if not last:

            def keep():
                ends[number + 1] = ends[number]

            guarded(place < hop, keep)
            guarded(place + 2 * hop < sp, states[number + 1].start)

    for number in range(1, parts_of - 1):
        relay(number, level < count - 1)
    relay(parts_of - 1)

    def arrive(names, last):
        for source in range(count):
            for side in range(2):
                slot = 2 * source + side

                def one(slot=slot):
                    for head in names:
                        for number in range(parts_of):
                            crossing(head, slot, number).wait_recv()

                guarded((lax.rem(place, 2) != side) & (slot <= last), one)

    part = rows // tp
    mate = swapped(me, 1)

    def lines(owner):
        return pl.ds(pl.multiple_of(owner * part, part), part)

    answers, gives, tells = [], [], []
    if moving:
        for turn in range(tp):
            owner = swapped(me, turn)
            answers.append(
                remote(
                    mix_far.at[:, lines(owner)],
                    bmix.at[turn],
                    b_send.at[turn],
                    b_recv.at[turn],
                    {"sp": mirror, "tp": owner} if turn else {"sp": mirror},
                )
            )
            if turn:
                gives.append(
                    remote(
                        mix.at[pl.ds(pairs + moving[0], len(moving)), lines(owner)],
                        bmix.at[turn],
                        g_send.at[turn],
                        b_recv.at[turn],
                        {"tp": owner},
                    )
                )
        tells.append(
            remote(log_far, log_got, l_send.at[0], l_recv.at[0], {"sp": mirror})
        )
    work = (queries, top, row_sum, acc)

    state[...] = jnp.zeros(state.shape, F32)
    scan(0)
    for number in range(1, len(scans) - 1):
        guarded(early, lambda number=number: scan(number))
    pl.when(early)(lambda: finish_body(heard, turned, state, mix))
    arrive(staying, place)
    for head in staying:
        attend(
            q.at[head], kv, head, place, lam[head], *work, mix.at[pairs + head], logs.at[head]
        )
    for number in range(1, len(scans) - 1):
        guarded(late, lambda number=number: scan(number))
    if len(scans) > 1:
        scan(len(scans) - 1)
    pl.when(late)(lambda: finish_body(heard, turned, state, mix))
    blocks = pairs + len(staying)
    swaps = []
    for turn in range(tp // 2):
        theirs = lines(lax.rem(mate + 2 * turn, tp))
        swaps.append(
            remote(
                mix.at[pl.ds(0, blocks), theirs],
                moved.at[:, theirs],
                m_send.at[turn],
                m_recv.at[turn],
                {"tp": mate},
            )
        )
    for one in swaps:
        one.start()
    owners = [lax.rem(me + 2 * turn, tp) for turn in range(1, tp // 2)] + [me]
    near = jnp.concatenate(
        [
            jnp.concatenate([mix[b, lines(owner), :] for b in range(blocks)], axis=1)
            for owner in owners
        ],
        axis=0,
    )
    slabs, slab = parts.shape[1], parts.shape[3]
    begun = [
        jnp.dot(near, hw[0, :, pl.ds(number * slab, slab)], preferred_element_type=F32)
        for number in range(slabs)
    ]
    outs.wait_recv()
    for one in swaps:
        one.wait_recv()
    far = jnp.concatenate(
        [
            jnp.concatenate([moved[b, lines(owner), :] for b in range(blocks)], axis=1)
            for owner in owners
        ],
        axis=0,
    )
    trades = {}
    for number in range(slabs):
        columns = pl.ds(number * slab, slab)
        result = begun[number] + jnp.dot(
            far, hw[1, :, columns], preferred_element_type=F32
        )
        for turn in range(1, tp // 2):
            parts[turn, number] = result[(turn - 1) * part : turn * part].astype(BF16)
            trades[turn, number] = remote(
                parts.at[turn, number],
                got.at[turn, number],
                p_send.at[turn, number],
                p_recv.at[turn, number],
                {"tp": lax.rem(me + 2 * turn, tp)},
            )
            trades[turn, number].start()
        total[:, columns] = result[(tp // 2 - 1) * part :]
    if moving:
        spreads[1].wait_recv()
        for turn in range(2, tp, 2):
            spreads[turn].wait_recv()
            spreads[turn + 1].start()
    if moving:

        def foreign():
            arrive(moving, mirror)
            for n, head in enumerate(moving):
                asks[n].wait_recv()
                attend(
                    q_far.at[n], kv, head, mirror, lam[head], *work, mix_far.at[n], log_far.at[n]
                )
            for one in answers + tells:
                one.start()

        guarded(early, foreign)
    if moving:

        def local():
            for head in moving:
                attend(
                    q.at[head],
                    kv,
                    head,
                    place,
                    lam[head],
                    *work,
                    mix.at[pairs + head],
                    logs.at[head],
                )
            for one in gives:
                one.start()
            for n, head in enumerate(moving):
                bmix[0, n] = mix[pairs + head, lines(me), :]
            for one in gives:
                one.wait_recv()

        def collect():
            for one in answers + tells:
                one.wait_recv()
            for n, head in enumerate(moving):
                logs[head] = log_got[n]

        guarded(early, local)
        guarded(late, collect)
    if moving:
        for turn in range(3, tp, 2):
            spreads[turn].wait_recv()
        beside = jnp.concatenate(
            [bmix[turn, n] for turn in range(tp) for n in range(len(moving))], axis=1
        )
    for number in range(slabs):
        columns = pl.ds(number * slab, slab)
        full = total[:, columns]
        if moving:
            weights = jnp.concatenate([wb[turn, :, columns] for turn in range(tp)], axis=0)
            full = full + jnp.dot(beside, weights, preferred_element_type=F32)
        for turn in range(1, tp // 2):
            trades[turn, number].wait_recv()
            full = full + got[turn, number].astype(F32)
        total[:, columns] = full
    full = total[...]
    mean = jnp.mean(full * full, axis=-1, keepdims=True)
    out[...] = (full * lax.rsqrt(mean + NORM_EPS) * out_gain[...]).astype(BF16)

    for group_of in (hops, trades, spreads):
        for one in group_of.values():
            one.wait_send()
    for one in swaps:
        one.wait_send()
    outs.wait_send()
    for number in range(parts_of):
        for head, condition in own_crosses:
            guarded(condition, crossing(head, place, number).wait_send)
        for head, target, condition in column_goes():
            guarded(condition, column(head, place, target, number).wait_send)
    for head, source, condition in relayed:

        def one(head=head, source=source):
            for number in range(parts_of):
                slot = 2 * source + lax.rem(place, 2)
                crossing(head, slot, number).wait_send()

        guarded(condition, one)
    for number, hop in enumerate(scans):
        guarded(place + hop < sp, states[number].wait_send)
    if moving:
        guarded(late, lambda: [one.wait_send() for one in asks] and None)
        guarded(early, lambda: [one.wait_send() for one in answers + gives + tells] and None)


def per_device(
    sp,
    tp,
    hidden_in,
    in_gain,
    receptance_weight,
    key_weight,
    value_weight,
    decay_down,
    decay_up,
    decay_base,
    decay_shift,
    learn_rate,
    query_pair,
    key_pair,
    value_pair,
    mix_lambda,
    out_recurrent,
    out_attention,
    out_gain,
):
    rows, width = hidden_in.shape
    depth = width * tp
    features = receptance_weight.shape[1]
    heads = mix_lambda.shape[0]
    wide = heads * LANES
    pairs = features // LANES
    low = decay_down.shape[1]
    across = out_recurrent.shape[1]
    part = rows // tp
    count = sp // 2
    movers = max(heads // 2, 1)
    stay = (heads - heads // 2) * LANES
    gone = max(wide - stay, 16)
    pieces = rows // LANES
    slabs = 4 if across % (4 * LANES) == 0 else 1
    shape = jax.ShapeDtypeStruct
    held = pltpu.VMEM

    def paired(weight):
        return weight.reshape(depth * heads, LANES)

    args = (
        hidden_in,
        in_gain.reshape(1, -1),
        receptance_weight,
        key_weight,
        value_weight,
        decay_down,
        decay_up,
        decay_base.reshape(1, -1),
        decay_shift,
        learn_rate.reshape(1, -1),
        paired(query_pair),
        paired(key_pair),
        paired(value_pair),
        mix_lambda,
        out_recurrent,
        out_attention,
        out_gain.reshape(1, -1),
    )
    inside = pl.BlockSpec(memory_space=pltpu.VMEM)
    outside = pl.BlockSpec(memory_space=pl.ANY)
    specs = [inside] * 2 + [outside] * 5 + [inside] * 3 + [outside] * 3
    specs += [pl.BlockSpec(memory_space=pltpu.SMEM)] + [outside] * 2 + [inside]
    raw = (depth * heads, LANES) if heads > 1 else (16, LANES)
    scans = max((sp - 1).bit_length(), 1)
    sizes = ((11,), (tp, pieces), (tp, pieces), (tp,), (tp,))
    sizes += ((heads, count, pieces),) * 4
    sizes += ((scans,), (scans,), (movers,), (movers,), (tp,), (tp,))
    sizes += ((tp // 2,), (tp // 2,), (tp // 2, slabs), (tp // 2, slabs))
    sizes += ((tp,), (1,), (1,))
    made = tuple(
        pl.pallas_call(
            functools.partial(layer_body, sp, tp),
            out_shape=[pltpu.VMEM((part, across), BF16), pltpu.VMEM((heads, 2, rows), F32)],
            in_specs=specs,
            out_specs=[inside] * 2,
            scratch_shapes=[
                held((tp, rows, width), BF16),
                held((rows, depth), BF16),
                held((depth, features), BF16),
                held((depth, features), BF16),
                held((depth, features), BF16),
                held((depth, low), BF16),
                held((low, features), BF16),
                held((depth, wide), BF16),
                held((depth, wide), BF16),
                held((depth, wide), BF16),
                held((2, features + stay, across), BF16),
                held((tp, gone, across), BF16),
                held((tp, movers, part, LANES), BF16),
                held(raw, BF16),
                held(raw, BF16),
                held(raw, BF16),
                held(raw, F32),
                held((sp, heads, pieces, 2 * LANES, LANES), BF16),
                held((rows, features), BF16),
                held((rows, features), BF16),
                held((rows, features), BF16),
                held((rows, features), F32),
                held((heads, rows, LANES), BF16),
                held((rows, features), F32),
                held((rows, features), F32),
                held((scans, pairs, 2 * HD, LANES), BF16),
                held((scans, pairs, 2 * HD, LANES), BF16),
                held((pairs, 2 * LANES, LANES), F32),
                held((pieces, 2 * LANES, LANES), BF16),
                held((pieces, 1, 2 * LANES), F32),
                held((pieces, 1, 2 * LANES), F32),
                held((pieces, LANES, 2 * LANES), F32),
                held((pairs + heads, rows, LANES), BF16),
                held((pairs + heads - heads // 2, rows, LANES), BF16),
                held((movers, rows, LANES), BF16),
                held((movers, rows, LANES), BF16),
                held((movers, 2, rows), F32),
                held((movers, 2, rows), F32),
                held((part, across), F32),
                held((tp // 2, slabs, part, across // slabs), BF16),
                held((tp // 2, slabs, part, across // slabs), BF16),
            ]
            + [pltpu.SemaphoreType.DMA(size) for size in sizes],
            compiler_params=pltpu.CompilerParams(
                collective_id=0, has_side_effects=True, vmem_limit_bytes=62 * 1024 * 1024
            ),
        )(*args)
    )
    return tuple(
        pl.pallas_call(
            settle_body,
            out_shape=[shape((part, across), BF16), shape((heads, 2, rows), F32)],
            in_specs=[outside] * 2,
            out_specs=[outside] * 2,
            scratch_shapes=[pltpu.SemaphoreType.DMA((2,))],
            compiler_params=pltpu.CompilerParams(vmem_limit_bytes=1024 * 1024),
        )(*made)
    )


def solution(mesh):
    in_specs = (
        P("sp", "tp"),
        P(),
        P(None, "tp"),
        P(None, "tp"),
        P(None, "tp"),
        P(),
        P(None, "tp"),
        P("tp"),
        P("sp", "tp"),
        P("tp"),
        P(None, "tp", None),
        P(None, "tp", None),
        P(None, "tp", None),
        P("tp"),
        P("tp", None),
        P("tp", None),
        P(),
    )
    out_specs = (P(("sp", "tp"), None), P("tp", None, "sp"))
    body = functools.partial(per_device, mesh.shape["sp"], mesh.shape["tp"])
    return jax.shard_map(
        body, mesh=mesh, in_specs=in_specs, out_specs=out_specs, check_vma=False
    )
```
